32 devices in a mesh: dp: 4 (over y, x), kv: 4 (over z), tp: 2 (over core).
Axes of the slice: x: 2, y: 2, z: 4, core: 2. Of those that a mesh axis runs over, the one named last changes fastest.
Arguments:
- tokens: bfloat16 [128, 2048], P('dp', 'kv'), may hold values from -18 to 18
- mix_gain: float32 [2048], P('kv'), may hold values from 0.1 to 1.9
- w_query: bfloat16 [2048, 1024], P('kv', 'tp'), may hold values from -0.125 to 0.125
- w_key: bfloat16 [2048, 1024], P('kv', 'tp'), may hold values from -0.125 to 0.125
- w_value: bfloat16 [2048, 2048], P('kv', 'tp'), may hold values from -0.125 to 0.125
- w_outgate: bfloat16 [2048, 2048], P('kv', 'tp'), may hold values from -0.125 to 0.125
- w_gates: bfloat16 [2048, 16], replicated, may hold values from -0.25 to 0.25
- forget_bias: float32 [8], P('tp'), may hold values from -1 to 3
- memory: float32 [128, 8, 128, 256], P(('dp', 'kv'), 'tp'), may hold values from -4 to 4
- normalizer: float32 [128, 8, 128], P(('dp', 'kv'), 'tp'), may hold values from -4 to 4
- stabilizer: float32 [128, 8], P(('dp', 'kv'), 'tp'), may hold values from -4 to 4
- head_gain: float32 [8, 256], P('tp'), may hold values from 0.1 to 1.9
- w_out: bfloat16 [2048, 2048], P('tp', 'kv'), may hold values from -0.125 to 0.125
- mlp_gain: float32 [2048], replicated, may hold values from 0.1 to 1.9
- w_gate: bfloat16 [2048, 5632], P(None, ('kv', 'tp')), may hold values from -0.125 to 0.125
- w_up: bfloat16 [2048, 5632], P(None, ('kv', 'tp')), may hold values from -0.125 to 0.125
- w_down: bfloat16 [5632, 2048], P(('kv', 'tp')), may hold values from -0.109375 to 0.109375
Outputs:
- mixed_out: bfloat16 [128, 2048], P('dp', ('kv', 'tp'))
- new_memory: float32 [128, 8, 128, 256], P(('dp', 'kv'), 'tp')
- new_normalizer: float32 [128, 8, 128], P(('dp', 'kv'), 'tp')
- new_stabilizer: float32 [128, 8], P(('dp', 'kv'), 'tp')
The draws below stay inside these ranges and needn't reach their ends.
All inputs are finite; a program needn't handle non-finite values.
Results may differ from the reference program's by a relative error of at most 0.02.
Values may be sent and summed in bfloat16 or wider, within the bound.
A program may use at most 64 MiB of HBM per device.

```python
import math
import jax
import jax.numpy as jnp
from jax import lax

D = 2048
HEADS = 8
QK = 128
VD = 256
FF = 5632
BATCH = 128
N_TP = 2


def draw_tokens(key, part):
    normal_key = jax.random.fold_in(jax.random.fold_in(key, 11), 0)
    columns = jnp.exp(jnp.linspace(0.0, math.log(3.0), D)).astype(jnp.float32)
    values_drawn = jnp.clip(jax.random.normal(normal_key, (BATCH, D), jnp.float32), -4.0, 4.0)
    return (values_drawn * columns).astype(jnp.bfloat16)


def strengthened(entries, stream_key, source, target, parts, factor):
    def block_of(dim):
        return (jnp.arange(entries.shape[dim]) // (entries.shape[dim] // parts)).reshape((-1,) + (1,) * (entries.ndim - 1 - dim))

    near = jax.random.permutation(stream_key, parts)[block_of(target)]
    far = (block_of(target) + parts // 2) % parts
    return jnp.where((block_of(source) == near) | (block_of(source) == far), factor * entries, entries)


def level_of(key, dims, cuts, least, largest):
    level, own = 1.0, jax.random.fold_in(key, 6)
    for axis_at, shards_of in cuts:
        heights = jnp.exp(jax.random.uniform(jax.random.fold_in(own, axis_at), (shards_of,), jnp.float32, least / len(cuts), largest / len(cuts)))
        level = level * jnp.repeat(heights, dims[axis_at] // shards_of).reshape([-1 if axis == axis_at else 1 for axis in range(len(dims))])
    return level


def centred(key, dims, width, bound, cuts=(), held_as=jnp.bfloat16):
    array = width * jax.random.normal(key, dims, jnp.float32)
    if cuts:
        array = array * level_of(key, dims, cuts, -0.22, 0.18)
    return jnp.clip(array, -bound, bound).astype(held_as)


def heavy_noise(stream_key, dims, scale, reach, shards, heavy, kind=jnp.bfloat16):
    values = scale * jax.random.normal(stream_key, dims, jnp.float32)
    if shards:
        values = values * level_of(stream_key, dims, shards, -0.22, 0.18)
    return jnp.clip(strengthened(values, jax.random.fold_in(stream_key, 3), *heavy), -reach, reach).astype(kind)


def setup_inputs(seed: int = 0) -> dict:
    arg_keys = jax.random.split(jax.random.key(seed), 18)
    tokens = draw_tokens(jax.random.fold_in(arg_keys[17], 71), 0)
    mix_gain = jnp.clip(1.0 + 0.18 * jax.random.normal(arg_keys[1], (D,), jnp.float32), 0.1, 1.9)
    w_query = centred(arg_keys[2], (D, HEADS * QK), D ** -0.5, 0.125, ((0, 4), (1, 2)))
    w_key = centred(arg_keys[3], (D, HEADS * QK), D ** -0.5, 0.125, ((0, 4), (1, 2)))
    w_value = centred(arg_keys[4], (D, HEADS * VD), D ** -0.5, 0.125, ((0, 4), (1, 2)))
    w_outgate = centred(arg_keys[5], (D, HEADS * VD), D ** -0.5, 0.125, ((0, 4), (1, 2)))
    w_gates = centred(arg_keys[6], (D, 2 * HEADS), (D // 4) ** -0.5, 0.25)
    forget_bias = jnp.clip(-1.0 + 4.0 * jax.random.uniform(arg_keys[7], (HEADS,), jnp.float32) ** level_of(arg_keys[7], (HEADS,), ((0, 2),), -0.2, 0.2), -1.0, 3.0)
    memory = centred(arg_keys[8], (BATCH, HEADS, QK, VD), 0.5, 4.0, ((0, 16), (1, 2)), jnp.float32)
    normalizer = centred(arg_keys[9], (BATCH, HEADS, QK), 0.5, 4.0, ((0, 16), (1, 2)), jnp.float32)
    stabilizer = centred(arg_keys[10], (BATCH, HEADS), 1.0, 4.0, ((0, 16), (1, 2)), jnp.float32)
    head_gain = jnp.clip(1.0 + 0.18 * jax.random.normal(arg_keys[11], (HEADS, VD), jnp.float32), 0.1, 1.9)
    w_out = centred(arg_keys[12], (HEADS * VD, D), (HEADS * VD) ** -0.5, 0.125, ((0, 2), (1, 4)))
    mlp_gain = jnp.clip(1.0 + 0.18 * jax.random.normal(arg_keys[13], (D,), jnp.float32), 0.1, 1.9)
    w_gate = centred(arg_keys[14], (D, FF), D ** -0.5, 0.125, ((1, 8),))
    w_up = centred(arg_keys[15], (D, FF), D ** -0.5, 0.125, ((1, 8),))
    w_down = heavy_noise(arg_keys[16], (FF, D), FF ** -0.5, 0.109375, ((0, 8),), (0, 1, 8, 2.0))
    return {"tokens": tokens, "mix_gain": mix_gain, "w_query": w_query, "w_key": w_key, "w_value": w_value, "w_outgate": w_outgate, "w_gates": w_gates, "forget_bias": forget_bias, "memory": memory, "normalizer": normalizer, "stabilizer": stabilizer, "head_gain": head_gain, "w_out": w_out, "mlp_gain": mlp_gain, "w_gate": w_gate, "w_up": w_up, "w_down": w_down}


EPSILON = 1e-06

def reference(tokens, mix_gain, w_query, w_key, w_value, w_outgate, w_gates, forget_bias, memory, normalizer, stabilizer, head_gain, w_out, mlp_gain, w_gate, w_up, w_down):
    activations = tokens.astype(jnp.float32)
    batch_rows = tokens.shape[0]
    inverse = lax.rsqrt(lax.optimization_barrier(jnp.mean(activations * activations, axis=1, keepdims=True)) + EPSILON)
    scaled = (activations * mix_gain).astype(jnp.bfloat16)
    query_rows = (jnp.dot(scaled, w_query, preferred_element_type=jnp.float32) * inverse).astype(jnp.bfloat16)
    key_rows = (jnp.dot(scaled, w_key, preferred_element_type=jnp.float32) * (inverse * QK ** (-0.5))).astype(jnp.bfloat16)
    value_rows = (jnp.dot(scaled, w_value, preferred_element_type=jnp.float32) * inverse).astype(jnp.bfloat16)
    outgate = (jnp.dot(scaled, w_outgate, preferred_element_type=jnp.float32) * inverse).astype(jnp.bfloat16)
    gate_pre = jnp.dot(scaled, w_gates, preferred_element_type=jnp.float32) * inverse
    input_pre = gate_pre[:, :HEADS]
    log_forget = jax.nn.log_sigmoid(gate_pre[:, HEADS:] + forget_bias)
    new_stabilizer = jnp.maximum(log_forget + stabilizer, input_pre)
    forget_scale = jnp.exp(log_forget + stabilizer - new_stabilizer)
    input_scale = jnp.exp(input_pre - new_stabilizer)
    query_heads = query_rows.astype(jnp.float32).reshape(batch_rows, HEADS, QK)
    key_heads = key_rows.astype(jnp.float32).reshape(batch_rows, HEADS, QK)
    value_heads = value_rows.astype(jnp.float32).reshape(batch_rows, HEADS, VD)
    new_normalizer = forget_scale[..., None] * normalizer + input_scale[..., None] * key_heads
    denominator = lax.optimization_barrier(jnp.sum(query_heads * new_normalizer, axis=2))
    carried = jnp.einsum('bhd,bhde->bhe', query_heads, memory, precision=lax.Precision.HIGHEST)
    query_key = lax.optimization_barrier(jnp.sum(query_heads * key_heads, axis=2))
    numerator = forget_scale[..., None] * carried + (input_scale * query_key)[..., None] * value_heads
    new_memory = forget_scale[..., None, None] * memory + (input_scale[..., None] * key_heads)[..., None] * value_heads[:, :, None, :]
    head_out = numerator / jnp.maximum(jnp.abs(denominator), 1.0)[..., None]
    normed = head_out * lax.rsqrt(lax.optimization_barrier(jnp.mean(head_out * head_out, axis=2, keepdims=True)) + EPSILON) * head_gain
    mixed_heads = (normed.reshape(batch_rows, HEADS * VD) * jax.nn.sigmoid(outgate.astype(jnp.float32))).astype(jnp.bfloat16)
    group_width = HEADS * VD // N_TP
    branch = jnp.zeros((batch_rows, D), jnp.float32)
    for group in range(N_TP):
        partial_out = jnp.dot(mixed_heads[:, group * group_width:(group + 1) * group_width], w_out[group * group_width:(group + 1) * group_width], preferred_element_type=jnp.float32).astype(jnp.bfloat16)
        branch = branch + lax.optimization_barrier(partial_out).astype(jnp.float32)
    residual = (activations + branch).astype(jnp.bfloat16)
    resid_float = residual.astype(jnp.float32)
    inverse_two = lax.rsqrt(lax.optimization_barrier(jnp.mean(resid_float * resid_float, axis=1, keepdims=True)) + EPSILON)
    mlp_in = (resid_float * inverse_two * mlp_gain).astype(jnp.bfloat16)
    gate_value = jnp.dot(mlp_in, w_gate, preferred_element_type=jnp.float32)
    up_value = jnp.dot(mlp_in, w_up, preferred_element_type=jnp.float32)
    hidden = (jax.nn.silu(gate_value) * up_value).astype(jnp.bfloat16)
    mixed_out = (jnp.dot(hidden, w_down, preferred_element_type=jnp.float32) + resid_float).astype(jnp.bfloat16)
    return (mixed_out, new_memory, new_normalizer, new_stabilizer)
```

```python
import functools

import jax
import jax.numpy as jnp
from jax import lax
from jax.experimental import pallas as pl
from jax.experimental.pallas import tpu as pltpu
from jax.sharding import PartitionSpec as P

QK = 128
VD = 256
EPSILON = 1e-06
MESH = pl.DeviceIdType.MESH
F32 = jnp.float32
BF16 = jnp.bfloat16


def dot(a, b):
    return jnp.dot(a, b, preferred_element_type=F32)


def dot_rows(a, b):
    return lax.dot_general(a, b, (((1,), (1,)), ((), ())), preferred_element_type=F32)


def nearest(rank, me, size):
    inner = jnp.minimum(me, size - 1 - me)
    close = me + ((rank + 1) // 2 if rank % 2 else -(rank // 2))
    beyond = (rank - inner) * jnp.where(2 * me < size - 1, 1, -1)
    return jnp.where(rank <= 2 * inner, close, me + beyond)


def layer_kernel(
    kv_size,
    tp_size,
    tokens_in,
    mix_gain_in,
    w_query,
    w_key,
    w_value,
    w_outgate,
    w_gates,
    forget_bias_in,
    memory,
    normalizer_in,
    stabilizer_in,
    head_gain_in,
    w_out,
    mlp_gain_in,
    w_gate,
    w_up,
    w_down,
    out_mixed,
    vmem,
    out_normalizer,
    out_stabilizer,
    vq,
    vk,
    vv,
    vo,
    vgates,
    tokens,
    mix_gain,
    forget_bias,
    normalizer,
    stabilizer,
    head_gain,
    mlp_gain,
    vwout,
    vgate,
    vup,
    vdown,
    send_qk,
    send_vo,
    send_gs,
    recv_qk,
    recv_vo,
    recv_gs,
    heads_all,
    branch_own,
    branch_recv,
    resid_all,
    gain_rows,
    down_pair,
    pair_recv,
    down_send,
    down_recv,
    load_sem,
    small_sem,
    send_sem,
    recv1,
    recv2,
    recv3,
    recv4,
    pair_sem,
    recv5,
):
    me = lax.axis_index("kv")
    core = lax.axis_index("tp")
    rows, cols = tokens.shape
    seq = rows // kv_size
    width = cols * kv_size
    local_heads = forget_bias.shape[1]
    total_heads = local_heads * tp_size
    half = local_heads * VD // 2
    group = kv_size * tp_size
    out_cols = width // group
    chunks = pair_recv.shape[1]
    chunk_chips = kv_size // chunks
    chunk_cols = width // chunks
    last = tp_size - 1

    barrier = pltpu.get_barrier_semaphore()
    rank = me * tp_size + core
    for step in range(1, group):
        other = lax.rem(rank + step, group)
        pl.semaphore_signal(
            barrier,
            inc=1,
            device_id={"kv": other // tp_size, "tp": lax.rem(other, tp_size)},
            device_id_type=MESH,
        )

    loads = [
        pltpu.make_async_copy(src, dst, load_sem.at[i])
        for i, (src, dst) in enumerate(
            (
                (w_gates.at[:, pl.ds(pl.multiple_of(me * cols, cols), cols)], vgates),
                (w_query, vq),
                (w_key, vk),
                (w_value, vv),
                (w_outgate, vo),
                (memory, vmem),
                (w_out, vwout),
                (w_gate, vgate),
                (w_up, vup),
                (w_down, vdown),
            )
        )
    ]
    small = [
        pltpu.make_async_copy(src, dst, small_sem.at[i])
        for i, (src, dst) in enumerate(
            (
                (tokens_in, tokens),
                (mix_gain_in, mix_gain),
                (mlp_gain_in, mlp_gain),
                (forget_bias_in, forget_bias),
                (normalizer_in, normalizer),
                (stabilizer_in, stabilizer),
                (head_gain_in, head_gain),
            )
        )
    ]
    for load in small[:2] + loads[:5] + small[2:]:
        load.start()

    def send(src, dst, index, recv_sem, device):
        pltpu.make_async_remote_copy(
            src_ref=src,
            dst_ref=dst,
            send_sem=send_sem.at[index],
            recv_sem=recv_sem,
            device_id=device,
            device_id_type=MESH,
        ).start()

    def drain(ref, sem):
        pltpu.make_async_copy(ref, ref, sem).wait()

    far_first = [nearest(k, me, kv_size) for k in range(kv_size - 1, 0, -1)]
    near_first = far_first[::-1]

    small[0].wait()
    small[1].wait()
    activations = tokens[...].astype(F32)
    square_part = jnp.sum(activations * activations, axis=1, keepdims=True)
    scaled = (activations * mix_gain[...]).astype(BF16)

    def stack_send(target, top, bottom):
        for block in range(kv_size):
            own = slice(block * seq, (block + 1) * seq)
            target[block] = jnp.concatenate([top[own], bottom[own]], axis=0).astype(BF16)

    def scatter(buffer, landing, kind):
        for target in far_first:
            send(buffer.at[target], landing.at[me], kind, recv1.at[kind, me], {"kv": target})

    loads[0].wait()
    gate_part = dot_rows(scaled, vgates[...])
    for block in range(kv_size):
        own = slice(block * seq, (block + 1) * seq)
        send_gs[block, :, 0 : 2 * total_heads] = gate_part[own]
        send_gs[block, :, 2 * total_heads : 2 * total_heads + 1] = square_part[own]
    loads[1].wait()
    query_part = dot(scaled, vq[...])
    loads[2].wait()
    key_part = dot(scaled, vk[...])
    stack_send(send_qk, query_part, key_part)
    pl.semaphore_wait(barrier, group - 1)
    scatter(send_gs, recv_gs, 0)
    scatter(send_qk, recv_qk, 1)
    loads[3].wait()
    value_part = dot(scaled, vv[...])
    loads[4].wait()
    outgate_part = dot(scaled, vo[...])
    stack_send(send_vo, value_part, outgate_part)

    def send_values():
        scatter(send_vo, recv_vo, 2)

    @pl.when(core == 0)
    def _():
        send_values()

    for load in loads[5:]:
        load.start()
    for load in small[2:]:
        load.wait()
    for block in range(kv_size):
        gain_rows[block] = mlp_gain[:, block * cols : (block + 1) * cols]

    def total(buffer, landing, kind):
        result = buffer[me].astype(F32)
        for source in near_first:
            drain(landing.at[source], recv1.at[kind, source])
            result = result + landing[source].astype(F32)
        return result

    gate_sum = total(send_gs, recv_gs, 0)

    @pl.when(core != 0)
    def _():
        send_values()

    inverse = lax.rsqrt(gate_sum[:, 2 * total_heads : 2 * total_heads + 1] / width + EPSILON)
    gate_pre = gate_sum[:, : 2 * total_heads] * inverse

    def own_columns(start):
        picked = gate_pre[:, start : start + local_heads]
        for other in range(1, tp_size):
            first = start + other * local_heads
            picked = jnp.where(core == other, gate_pre[:, first : first + local_heads], picked)
        return picked

    input_pre = own_columns(0)
    forget_pre = own_columns(total_heads) + forget_bias[...]
    log_forget = jnp.minimum(forget_pre, 0.0) - jnp.log1p(jnp.exp(-jnp.abs(forget_pre)))
    carried_log = log_forget + stabilizer[...].T
    new_stabilizer = jnp.maximum(carried_log, input_pre)
    out_stabilizer[...] = new_stabilizer.T
    forget_scale = jnp.exp(carried_log - new_stabilizer)
    input_scale = jnp.exp(input_pre - new_stabilizer)

    qk_sum = total(send_qk, recv_qk, 1)
    query = (qk_sum[:seq] * inverse).astype(BF16).astype(F32)
    key = (qk_sum[seq:] * (inverse * QK ** (-0.5))).astype(BF16).astype(F32)
    loads[5].wait()
    states = []
    for head in range(local_heads):
        span = slice(head * QK, (head + 1) * QK)
        q, k = query[:, span], key[:, span]
        forget, gain = forget_scale[:, head : head + 1], input_scale[:, head : head + 1]
        scaled_key = gain * k
        new_norm = forget * normalizer[:, head, :] + scaled_key
        out_normalizer[:, head, :] = new_norm
        denominator = jnp.sum(q * new_norm, axis=1, keepdims=True)
        query_key = jnp.sum(q * k, axis=1, keepdims=True)
        q_columns = q.T
        carried = jnp.concatenate(
            [
                jnp.sum(q_columns[:, b : b + 1] * vmem[b, head], axis=0, keepdims=True)
                for b in range(seq)
            ],
            axis=0,
        )
        states.append((forget, gain, scaled_key, denominator, query_key, carried))

    vo_sum = total(send_vo, recv_vo, 2)
    values = (vo_sum[:seq] * inverse).astype(BF16).astype(F32)
    outgate = (vo_sum[seq:] * inverse).astype(BF16).astype(F32)
    mixed = []
    for head in range(local_heads):
        forget, gain, scaled_key, denominator, query_key, carried = states[head]
        span = slice(head * VD, (head + 1) * VD)
        numerator = forget * carried + (gain * query_key) * values[:, span]
        head_out = numerator / jnp.maximum(jnp.abs(denominator), 1.0)
        normed = (
            head_out
            * lax.rsqrt(jnp.mean(head_out * head_out, axis=1, keepdims=True) + EPSILON)
            * head_gain[head : head + 1, :]
        )
        mixed.append(normed * jax.nn.sigmoid(outgate[:, span]))
    mixed = jnp.concatenate(mixed, axis=1)
    heads_all[me] = jnp.concatenate([mixed[:, :half], mixed[:, half:]], axis=0).astype(BF16)
    for target in far_first:
        send(heads_all.at[me], heads_all.at[me], 3, recv2.at[me], {"kv": target})

    for head in range(local_heads):
        forget, gain, scaled_key, denominator, query_key, carried = states[head]
        k_columns = scaled_key.T
        forget_rows = jnp.broadcast_to(forget, (seq, VD))
        for b in range(seq):
            vmem[b, head] = (
                forget_rows[b : b + 1] * vmem[b, head]
                + k_columns[:, b : b + 1] * values[b : b + 1, head * VD : (head + 1) * VD]
            )

    loads[6].wait()
    for source in near_first:
        drain(heads_all.at[source], recv2.at[source])
    gathered = [heads_all[block].astype(F32) for block in range(kv_size)]
    low = jnp.concatenate([g[:seq] for g in gathered], axis=0).astype(BF16)
    high = jnp.concatenate([g[seq:] for g in gathered], axis=0).astype(BF16)
    branch_own[...] = (dot(low, vwout[:half, :]) + dot(high, vwout[half:, :])).astype(BF16)

    @pl.when(core != 0)
    def _():
        send(branch_own, branch_recv.at[core - 1], 4, recv3.at[core - 1], {"tp": 0})

    @pl.when(core == 0)
    def _():
        branch = branch_own[...].astype(F32)
        for other in range(tp_size - 1):
            drain(branch_recv.at[other], recv3.at[other])
            branch = branch + branch_recv[other].astype(F32)
        resid_all[me] = (activations + branch).astype(BF16)
        for target in far_first:
            send(resid_all.at[me], resid_all.at[me], 4, recv4.at[me], {"kv": target})

    def pass_on(source):
        for other in range(1, tp_size):
            send(
                resid_all.at[source],
                resid_all.at[source],
                5,
                recv4.at[source],
                {"tp": other},
            )

    loads[7].wait()
    loads[8].wait()
    gate_value = up_value = square_sum = 0.0
    for source in [me] + near_first:
        @pl.when(core == 0)
        def _():
            if source is not me:
                drain(resid_all.at[source], recv4.at[source])
            pass_on(source)

        @pl.when(core != 0)
        def _():
            drain(resid_all.at[source], recv4.at[source])

        block = resid_all[source].astype(F32)
        square_sum = square_sum + jnp.sum(block * block, axis=1, keepdims=True)
        block = (block * gain_rows[source]).astype(BF16)
        span = pl.ds(pl.multiple_of(source * cols, cols), cols)
        gate_value = gate_value + dot_rows(block, vgate[:, span])
        up_value = up_value + dot_rows(block, vup[:, span])
    inverse_two = lax.rsqrt(square_sum / width + EPSILON)
    gate_value = gate_value * inverse_two
    up_value = up_value * inverse_two
    hidden = (gate_value * jax.nn.sigmoid(gate_value) * up_value).astype(BF16)

    loads[9].wait()
    upper = me >= kv_size // 2
    for step in range(chunks):
        chunk = jnp.where(upper, step, chunks - 1 - step) if chunks > 1 else 0
        span = pl.ds(pl.multiple_of(chunk * chunk_cols, chunk_cols), chunk_cols)
        part = dot(hidden, vdown[:, span])

        @pl.when(core != last)
        def _():
            down_pair[step] = part.astype(BF16)
            send(
                down_pair.at[step],
                pair_recv.at[core, step],
                6,
                pair_sem.at[core, step],
                {"tp": last},
            )

        @pl.when(core == last)
        def _():
            summed = part
            for other in range(last):
                drain(pair_recv.at[other, step], pair_sem.at[other, step])
                summed = summed + pair_recv[other, step].astype(F32)
            for chip in range(chunk_chips):
                for other in range(tp_size):
                    index = (chunk * chunk_chips + chip) * tp_size + other
                    first = (chip * tp_size + other) * out_cols
                    down_send[index] = summed[:, first : first + out_cols].astype(BF16)
            base = chunk * chunk_chips
            for place in range(chunk_chips):
                chip = base + jnp.where(upper, place, chunk_chips - 1 - place)
                for other in range(tp_size):
                    block = down_send.at[chip * tp_size + other]

                    @pl.when(chip != me)
                    def _():
                        send(
                            block,
                            down_recv.at[me],
                            6,
                            recv5.at[me],
                            {"kv": chip, "tp": other},
                        )

                    if other != last:
                        @pl.when(chip == me)
                        def _():
                            send(block, down_recv.at[me], 6, recv5.at[me], {"tp": other})

    @pl.when(core == last)
    def _():
        down_recv[me] = down_send[me * tp_size + last]

    @pl.when(core != last)
    def _():
        drain(down_recv.at[me], recv5.at[me])

    residual = resid_all[me].astype(F32)
    summed = down_recv[me].astype(F32) + residual[:, :out_cols]
    if tp_size > 1:
        own_residual = residual[:, :out_cols]
        for other in range(1, tp_size):
            own_residual = jnp.where(
                core == other, residual[:, other * out_cols : (other + 1) * out_cols], own_residual
            )
        summed = down_recv[me].astype(F32) + own_residual
    for source in near_first:
        drain(down_recv.at[source], recv5.at[source])
        summed = summed + down_recv[source].astype(F32)
    out_mixed[...] = summed.astype(BF16)
    peers = kv_size - 1
    drain(send_gs.at[:peers], send_sem.at[0])
    drain(send_qk.at[:peers], send_sem.at[1])
    drain(send_vo.at[:peers], send_sem.at[2])
    drain(heads_all.at[:peers], send_sem.at[3])

    @pl.when(core == 0)
    def _():
        drain(resid_all.at[:peers], send_sem.at[4])
        for _ in range(tp_size - 1):
            drain(resid_all, send_sem.at[5])

    @pl.when(core != 0)
    def _():
        drain(branch_own, send_sem.at[4])

    @pl.when(core == last)
    def _():
        drain(down_send.at[: group - 1], send_sem.at[6])

    @pl.when(core != last)
    def _():
        drain(down_pair, send_sem.at[6])


def store_kernel(mixed, memory, normalizer, stabilizer, *rest):
    sem = rest[-1]
    copies = [
        pltpu.make_async_copy(src, dst, sem.at[i])
        for i, (src, dst) in enumerate(zip((mixed, memory, normalizer, stabilizer), rest))
    ]
    for copy in copies:
        copy.start()
    for copy in copies:
        copy.wait()


def body(kv_size, tp_size, *args):
    (
        tokens,
        mix_gain,
        w_query,
        w_key,
        w_value,
        w_outgate,
        w_gates,
        forget_bias,
        memory,
        normalizer,
        stabilizer,
        head_gain,
        w_out,
        mlp_gain,
        w_gate,
        w_up,
        w_down,
    ) = args
    w_gates, w_gate, w_up, stabilizer = w_gates.T, w_gate.T, w_up.T, stabilizer.T
    rows, cols = tokens.shape
    local_heads, seq = stabilizer.shape
    group = kv_size * tp_size
    out_cols = cols // tp_size
    half = local_heads * VD // 2
    vmem = pl.BlockSpec(memory_space=pltpu.VMEM)
    hbm = pl.BlockSpec(memory_space=pl.ANY)
    width = cols * kv_size
    chunks = 2 if kv_size % 2 == 0 else 1

    def like(array):
        return pltpu.VMEM(array.shape, array.dtype)

    results = (
        ((rows, out_cols), BF16),
        (memory.shape, F32),
        (normalizer.shape, F32),
        (stabilizer.shape, F32),
    )
    gains = (mix_gain.reshape(1, cols), mlp_gain.reshape(1, mlp_gain.shape[0]))
    forget_bias = forget_bias.reshape(1, local_heads)
    held = pl.pallas_call(
        functools.partial(layer_kernel, kv_size, tp_size),
        out_shape=tuple(pltpu.VMEM(*result) for result in results),
        in_specs=[hbm] * len(args),
        out_specs=(vmem,) * len(results),
        scratch_shapes=[
            like(w_query),
            like(w_key),
            like(w_value),
            like(w_outgate),
            pltpu.VMEM((w_gates.shape[0], cols), BF16),
            like(tokens),
            like(gains[0]),
            like(forget_bias),
            like(normalizer),
            like(stabilizer),
            like(head_gain),
            like(gains[1]),
            like(w_out),
            like(w_gate),
            like(w_up),
            like(w_down),
            pltpu.VMEM((kv_size, 2 * seq, local_heads * QK), BF16),
            pltpu.VMEM((kv_size, 2 * seq, local_heads * VD), BF16),
            pltpu.VMEM((kv_size, seq, 128), F32),
            pltpu.VMEM((kv_size, 2 * seq, local_heads * QK), BF16),
            pltpu.VMEM((kv_size, 2 * seq, local_heads * VD), BF16),
            pltpu.VMEM((kv_size, seq, 128), F32),
            pltpu.VMEM((kv_size, 2 * seq, half), BF16),
            pltpu.VMEM((rows, cols), BF16),
            pltpu.VMEM((max(tp_size - 1, 1), rows, cols), BF16),
            pltpu.VMEM((kv_size, rows, cols), BF16),
            pltpu.VMEM((kv_size, 1, cols), F32),
            pltpu.VMEM((chunks, rows, width // chunks), BF16),
            pltpu.VMEM((max(tp_size - 1, 1), chunks, rows, width // chunks), BF16),
            pltpu.VMEM((group, rows, out_cols), BF16),
            pltpu.VMEM((kv_size, rows, out_cols), BF16),
            pltpu.SemaphoreType.DMA((10,)),
            pltpu.SemaphoreType.DMA((7,)),
            pltpu.SemaphoreType.DMA((7,)),
            pltpu.SemaphoreType.DMA((3, kv_size)),
            pltpu.SemaphoreType.DMA((kv_size,)),
            pltpu.SemaphoreType.DMA((max(tp_size - 1, 1),)),
            pltpu.SemaphoreType.DMA((kv_size,)),
            pltpu.SemaphoreType.DMA((max(tp_size - 1, 1), chunks)),
            pltpu.SemaphoreType.DMA((kv_size,)),
        ],
        compiler_params=pltpu.CompilerParams(
            collective_id=0, has_side_effects=True, vmem_limit_bytes=48 * 2**20
        ),
    )(*(pltpu.with_memory_space_constraint(x, pltpu.HBM) for x in (
        tokens,
        gains[0],
        w_query,
        w_key,
        w_value,
        w_outgate,
        w_gates,
        forget_bias,
        memory,
        normalizer,
        stabilizer,
        head_gain,
        w_out,
        gains[1],
        w_gate,
        w_up,
        w_down,
    )))
    mixed_out, new_memory, new_normalizer, new_stabilizer = pl.pallas_call(
        store_kernel,
        out_shape=tuple(jax.ShapeDtypeStruct(*result) for result in results),
        in_specs=[vmem] * len(results),
        out_specs=(hbm,) * len(results),
        scratch_shapes=[pltpu.SemaphoreType.DMA((len(results),))],
        compiler_params=pltpu.CompilerParams(vmem_limit_bytes=2**20),
    )(*held)
    return mixed_out, new_memory, new_normalizer, new_stabilizer.T


def solution(mesh):
    in_specs = (
        P("dp", "kv"),
        P("kv"),
        P("kv", "tp"),
        P("kv", "tp"),
        P("kv", "tp"),
        P("kv", "tp"),
        P(),
        P("tp"),
        P(("dp", "kv"), "tp", None, None),
        P(("dp", "kv"), "tp", None),
        P(("dp", "kv"), "tp"),
        P("tp", None),
        P("tp", "kv"),
        P(),
        P(None, ("kv", "tp")),
        P(None, ("kv", "tp")),
        P(("kv", "tp"), None),
    )
    out_specs = (
        P("dp", ("kv", "tp")),
        P(("dp", "kv"), "tp", None, None),
        P(("dp", "kv"), "tp", None),
        P(("dp", "kv"), "tp"),
    )
    return jax.shard_map(
        functools.partial(body, mesh.shape["kv"], mesh.shape["tp"]),
        mesh=mesh,
        in_specs=in_specs,
        out_specs=out_specs,
        check_vma=False,
    )
```

```python
import functools

import jax
import jax.numpy as jnp
from jax import lax
from jax.experimental import pallas as pl
from jax.experimental.pallas import tpu as pltpu
from jax.sharding import PartitionSpec as P

QK = 128
VD = 256
LANES = 128
EPSILON = 1e-06
MESH = pl.DeviceIdType.MESH
F32 = jnp.float32
BF16 = jnp.bfloat16


def dot(a, b):
    return jnp.dot(a, b, preferred_element_type=F32)


def dot_rows(a, b):
    return lax.dot_general(a, b, (((1,), (1,)), ((), ())), preferred_element_type=F32)


def nearest(rank, me, size):
    inner = jnp.minimum(me, size - 1 - me)
    away = rank // 2 + 1 if rank % 2 else -(rank // 2)
    away = jnp.where(rank <= 2 * inner, away, rank - inner)
    return jnp.where(2 * me < size - 1, me + away, me - away)


def layer_kernel(
    kv_size,
    tp_size,
    tokens_in,
    mix_gain_in,
    w_query,
    w_key,
    w_value,
    w_outgate,
    w_gates,
    forget_bias_in,
    memory,
    normalizer_in,
    stabilizer_in,
    head_gain_in,
    w_out,
    mlp_gain_in,
    w_gate,
    w_up,
    w_down,
    out_mixed,
    vmem,
    out_normalizer,
    out_stabilizer,
    vq,
    vk,
    vv,
    vo,
    vgates,
    tokens,
    mix_gain,
    forget_bias,
    normalizer,
    stabilizer,
    head_gain,
    mlp_gain,
    vwout,
    vgate,
    vup,
    vdown,
    send_qk,
    send_vo,
    send_gs,
    recv_qk,
    recv_vo,
    recv_gs,
    heads_all,
    branch_own,
    branch_recv,
    resid_all,
    gain_rows,
    gate_sum_ref,
    up_sum_ref,
    down_pair,
    pair_recv,
    down_send,
    down_recv,
    load_sem,
    small_sem,
    send_sem,
    recv1,
    recv2,
    recv3,
    recv4,
    pair_sem,
    recv5,
):
    me = lax.axis_index("kv")
    core = lax.axis_index("tp")
    rows, cols = tokens.shape
    seq = rows // kv_size
    width = cols * kv_size
    local_heads = forget_bias.shape[1]
    total_heads = local_heads * tp_size
    half = local_heads * VD // 2
    group = kv_size * tp_size
    out_cols = width // group
    lead = tp_size - 1
    sink = 0
    beside_lead = [(lead + 1 + i) % tp_size for i in range(tp_size - 1)]
    beside_sink = [(sink + 1 + i) % tp_size for i in range(tp_size - 1)]
    after_lead = lax.rem(core + tp_size - lead - 1 + tp_size, tp_size)
    after_sink = lax.rem(core + tp_size - sink - 1 + tp_size, tp_size)

    barrier = pltpu.get_barrier_semaphore()
    rank = me * tp_size + core
    for step in range(1, group):
        other = lax.rem(rank + step, group)
        pl.semaphore_signal(
            barrier,
            inc=1,
            device_id={"kv": other // tp_size, "tp": lax.rem(other, tp_size)},
            device_id_type=MESH,
        )

    loads = [
        pltpu.make_async_copy(src, dst, load_sem.at[i])
        for i, (src, dst) in enumerate(
            (
                (w_gates.at[:, pl.ds(pl.multiple_of(me * cols, cols), cols)], vgates),
                (w_query, vq),
                (w_key, vk),
                (w_value, vv),
                (w_outgate, vo),
                (memory, vmem),
                (w_out, vwout),
                (w_gate, vgate),
                (w_up, vup),
                (w_down, vdown),
            )
        )
    ]
    small = [
        pltpu.make_async_copy(src, dst, small_sem.at[i])
        for i, (src, dst) in enumerate(
            (
                (tokens_in, tokens),
                (mix_gain_in, mix_gain),
                (mlp_gain_in, mlp_gain),
                (forget_bias_in, forget_bias),
                (normalizer_in, normalizer),
                (stabilizer_in, stabilizer),
                (head_gain_in, head_gain),
            )
        )
    ]
    for load in small[:2] + loads[:5] + small[2:]:
        load.start()

    def send(src, dst, index, recv_sem, device):
        pltpu.make_async_remote_copy(
            src_ref=src,
            dst_ref=dst,
            send_sem=send_sem.at[index],
            recv_sem=recv_sem,
            device_id=device,
            device_id_type=MESH,
        ).start()

    def slot(source, target):
        return lax.rem(source - target + kv_size, kv_size) - 1

    def drain(ref, sem):
        pltpu.make_async_copy(ref, ref, sem).wait()

    far_first = [nearest(k, me, kv_size) for k in range(kv_size - 1, 0, -1)]
    near_first = far_first[::-1]
    outer = jnp.minimum(me, kv_size - 1 - me) < kv_size // 4
    ends_far_first = [jnp.where(outer, a, b) for a, b in zip(far_first, near_first)]

    small[0].wait()
    small[1].wait()
    activations = tokens[...].astype(F32)
    square_part = jnp.sum(activations * activations, axis=1, keepdims=True)
    scaled = (activations * mix_gain[...]).astype(BF16)

    def stack_send(target, top, bottom):
        for block in range(kv_size):
            own = slice(block * seq, (block + 1) * seq)
            target[block] = jnp.concatenate([top[own], bottom[own]], axis=0).astype(BF16)

    def scatter(buffer, landing, kind):
        for target in far_first:
            send(buffer.at[target], landing.at[me], kind, recv1.at[kind, slot(me, target)], {"kv": target})

    loads[0].wait()
    gate_part = dot_rows(scaled, vgates[...])
    for block in range(kv_size):
        own = slice(block * seq, (block + 1) * seq)
        send_gs[block, :, 0 : 2 * total_heads] = gate_part[own]
        send_gs[block, :, 2 * total_heads : 2 * total_heads + 1] = square_part[own]
    loads[1].wait()
    query_part = dot(scaled, vq[...])
    loads[2].wait()
    key_part = dot(scaled, vk[...])
    stack_send(send_qk, query_part, key_part)
    pl.semaphore_wait(barrier, group - 1)
    scatter(send_gs, recv_gs, 0)

    @pl.when(core == 0)
    def _():
        scatter(send_qk, recv_qk, 1)

    loads[3].wait()
    value_part = dot(scaled, vv[...])
    loads[4].wait()
    outgate_part = dot(scaled, vo[...])
    stack_send(send_vo, value_part, outgate_part)

    @pl.when(core == 0)
    def _():
        scatter(send_vo, recv_vo, 2)

    for load in loads[5:]:
        load.start()
    for load in small[2:]:
        load.wait()
    for block in range(kv_size):
        gain_rows[block] = mlp_gain[:, block * cols : (block + 1) * cols]

    def total(buffer, landing, kind):
        result = buffer[me].astype(F32)
        for source in near_first:
            drain(landing.at[source], recv1.at[kind, slot(source, me)])
            result = result + landing[source].astype(F32)
        return result

    gate_sum = total(send_gs, recv_gs, 0)

    inverse = lax.rsqrt(gate_sum[:, 2 * total_heads : 2 * total_heads + 1] / width + EPSILON)
    gate_pre = gate_sum[:, : 2 * total_heads] * inverse

    def own_columns(start):
        picked = gate_pre[:, start : start + local_heads]
        for other in range(1, tp_size):
            first = start + other * local_heads
            picked = jnp.where(core == other, gate_pre[:, first : first + local_heads], picked)
        return picked

    input_pre = own_columns(0)
    forget_pre = own_columns(total_heads) + forget_bias[...]
    log_forget = jnp.minimum(forget_pre, 0.0) - jnp.log1p(jnp.exp(-jnp.abs(forget_pre)))
    carried_log = log_forget + stabilizer[...].T
    new_stabilizer = jnp.maximum(carried_log, input_pre)
    out_stabilizer[...] = new_stabilizer.T
    forget_scale = jnp.exp(carried_log - new_stabilizer)
    input_scale = jnp.exp(input_pre - new_stabilizer)

    @pl.when(core != 0)
    def _():
        scatter(send_qk, recv_qk, 1)
        scatter(send_vo, recv_vo, 2)

    qk_sum = total(send_qk, recv_qk, 1)
    query = (qk_sum[:seq] * inverse).astype(BF16).astype(F32)
    key = (qk_sum[seq:] * (inverse * QK ** (-0.5))).astype(BF16).astype(F32)
    loads[5].wait()
    place = lax.broadcasted_iota(jnp.int32, (seq, seq * LANES), 1) // LANES
    spread = jnp.where(
        place == lax.broadcasted_iota(jnp.int32, (seq, seq * LANES), 0), 1.0, 0.0
    ).astype(BF16)
    states = []
    for head in range(local_heads):
        span = slice(head * QK, (head + 1) * QK)
        q, k = query[:, span], key[:, span]
        forget, gain = forget_scale[:, head : head + 1], input_scale[:, head : head + 1]
        scaled_key = gain * k
        new_norm = forget * normalizer[:, head, :] + scaled_key
        out_normalizer[:, head, :] = new_norm
        denominator = jnp.sum(q * new_norm, axis=1, keepdims=True)
        query_key = jnp.sum(q * k, axis=1, keepdims=True)
        q_lanes = dot(q.T.astype(BF16), spread)
        carried = jnp.concatenate(
            [
                jnp.concatenate(
                    [
                        jnp.sum(
                            q_lanes[:, b * LANES : (b + 1) * LANES]
                            * vmem[b, head, :, first : first + LANES],
                            axis=0,
                            keepdims=True,
                        )
                        for first in range(0, VD, LANES)
                    ],
                    axis=1,
                )
                for b in range(seq)
            ],
            axis=0,
        )
        states.append((forget, gain, scaled_key, denominator, query_key, carried))

    vo_sum = total(send_vo, recv_vo, 2)
    values = (vo_sum[:seq] * inverse).astype(BF16).astype(F32)
    outgate = (vo_sum[seq:] * inverse).astype(BF16).astype(F32)
    mixed = []
    for head in range(local_heads):
        forget, gain, scaled_key, denominator, query_key, carried = states[head]
        span = slice(head * VD, (head + 1) * VD)
        numerator = forget * carried + (gain * query_key) * values[:, span]
        head_out = numerator / jnp.maximum(jnp.abs(denominator), 1.0)
        normed = (
            head_out
            * lax.rsqrt(jnp.mean(head_out * head_out, axis=1, keepdims=True) + EPSILON)
            * head_gain[head : head + 1, :]
        )
        mixed.append(normed * jax.nn.sigmoid(outgate[:, span]))
    mixed = jnp.concatenate(mixed, axis=1)
    heads_all[me] = jnp.concatenate([mixed[:, :half], mixed[:, half:]], axis=0).astype(BF16)
    for target in far_first:
        send(heads_all.at[me], heads_all.at[me], 3, recv2.at[slot(me, target)], {"kv": target})

    for head in range(local_heads):
        forget, gain, scaled_key, denominator, query_key, carried = states[head]
        k_columns = scaled_key.T
        forget_rows = jnp.broadcast_to(forget, (seq, VD))
        for b in range(seq):
            vmem[b, head] = (
                forget_rows[b : b + 1] * vmem[b, head]
                + k_columns[:, b : b + 1] * values[b : b + 1, head * VD : (head + 1) * VD]
            )

    loads[6].wait()
    for source in near_first:
        drain(heads_all.at[source], recv2.at[slot(source, me)])
    gathered = [heads_all[block].astype(F32) for block in range(kv_size)]
    low = jnp.concatenate([g[:seq] for g in gathered], axis=0).astype(BF16)
    high = jnp.concatenate([g[seq:] for g in gathered], axis=0).astype(BF16)
    branch_own[...] = (dot(low, vwout[:half, :]) + dot(high, vwout[half:, :])).astype(BF16)

    @pl.when(core != lead)
    def _():
        send(branch_own, branch_recv.at[after_lead], 4, recv3.at[after_lead], {"tp": lead})

    @pl.when(core == lead)
    def _():
        branch = branch_own[...].astype(F32)
        for other in range(len(beside_lead)):
            drain(branch_recv.at[other], recv3.at[other])
            branch = branch + branch_recv[other].astype(F32)
        resid_all[me] = (activations + branch).astype(BF16)
        for target in ends_far_first:
            send(resid_all.at[me], resid_all.at[me], 4, recv4.at[me], {"kv": target})

    def pass_on(source):
        for other in beside_lead:
            send(
                resid_all.at[source],
                resid_all.at[source],
                5,
                recv4.at[source],
                {"tp": other},
            )

    loads[7].wait()
    loads[8].wait()
    square_sum = 0.0
    for source in [me] + near_first:
        @pl.when(core == lead)
        def _():
            if source is not me:
                drain(resid_all.at[source], recv4.at[source])
            pass_on(source)

        @pl.when(core != lead)
        def _():
            drain(resid_all.at[source], recv4.at[source])

        block = resid_all[source].astype(F32)
        square_sum = square_sum + jnp.sum(block * block, axis=1, keepdims=True)
        block = (block * gain_rows[source]).astype(BF16)
        span = pl.ds(pl.multiple_of(source * cols, cols), cols)
        if source is me:
            gate_sum_ref[...] = dot_rows(block, vgate[:, span])
            up_sum_ref[...] = dot_rows(block, vup[:, span])
        else:
            gate_sum_ref[...] += dot_rows(block, vgate[:, span])
            up_sum_ref[...] += dot_rows(block, vup[:, span])
    inverse_two = lax.rsqrt(square_sum / width + EPSILON)
    gate_value = gate_sum_ref[...] * inverse_two
    up_value = up_sum_ref[...] * inverse_two
    hidden = (gate_value * jax.nn.sigmoid(gate_value) * up_value).astype(BF16)

    loads[9].wait()
    for step, chip in enumerate(far_first + [me]):
        span = pl.ds(pl.multiple_of(chip * cols, cols), cols)
        part = dot(hidden, vdown[:, span])

        @pl.when(core != sink)
        def _():
            down_pair[step] = part.astype(BF16)
            send(
                down_pair.at[step],
                pair_recv.at[after_sink, step],
                6,
                pair_sem.at[after_sink, step],
                {"tp": sink},
            )

        @pl.when(core == sink)
        def _():
            summed = part
            for other in range(len(beside_sink)):
                drain(pair_recv.at[other, step], pair_sem.at[other, step])
                summed = summed + pair_recv[other, step].astype(F32)
            for other in range(tp_size):
                first = other * out_cols
                down_send[chip * tp_size + other] = summed[:, first : first + out_cols].astype(BF16)
            if chip is me:
                for other in beside_sink:
                    send(
                        down_send.at[me * tp_size + other],
                        down_recv.at[me],
                        6,
                        recv5.at[me],
                        {"tp": other},
                    )
            else:
                for other in range(tp_size):
                    send(
                        down_send.at[chip * tp_size + other],
                        down_recv.at[me],
                        6,
                        recv5.at[me],
                        {"kv": chip, "tp": other},
                    )

    @pl.when(core == sink)
    def _():
        down_recv[me] = down_send[me * tp_size + sink]

    @pl.when(core != sink)
    def _():
        drain(down_recv.at[me], recv5.at[me])

    residual = resid_all[me].astype(F32)
    summed = down_recv[me].astype(F32) + residual[:, :out_cols]
    if tp_size > 1:
        own_residual = residual[:, :out_cols]
        for other in range(1, tp_size):
            own_residual = jnp.where(
                core == other, residual[:, other * out_cols : (other + 1) * out_cols], own_residual
            )
        summed = down_recv[me].astype(F32) + own_residual
    for source in near_first:
        drain(down_recv.at[source], recv5.at[source])
        summed = summed + down_recv[source].astype(F32)
    out_mixed[...] = summed.astype(BF16)
    peers = kv_size - 1
    drain(send_gs.at[:peers], send_sem.at[0])
    drain(send_qk.at[:peers], send_sem.at[1])
    drain(send_vo.at[:peers], send_sem.at[2])
    drain(heads_all.at[:peers], send_sem.at[3])

    @pl.when(core == lead)
    def _():
        drain(resid_all.at[:peers], send_sem.at[4])
        for _ in range(tp_size - 1):
            drain(resid_all, send_sem.at[5])

    @pl.when(core != lead)
    def _():
        drain(branch_own, send_sem.at[4])

    @pl.when(core == sink)
    def _():
        drain(down_send.at[: group - 1], send_sem.at[6])

    @pl.when(core != sink)
    def _():
        drain(down_pair, send_sem.at[6])


def store_kernel(mixed, memory, normalizer, stabilizer, *rest):
    sem = rest[-1]
    pairs = [(memory.at[i], rest[1].at[i]) for i in range(memory.shape[0])]
    pairs += [(mixed, rest[0]), (normalizer, rest[2]), (stabilizer, rest[3])]
    copies = [
        pltpu.make_async_copy(src, dst, sem.at[i]) for i, (src, dst) in enumerate(pairs)
    ]
    for copy in copies:
        copy.start()
    for copy in copies:
        copy.wait()


def body(kv_size, tp_size, *args):
    (
        tokens,
        mix_gain,
        w_query,
        w_key,
        w_value,
        w_outgate,
        w_gates,
        forget_bias,
        memory,
        normalizer,
        stabilizer,
        head_gain,
        w_out,
        mlp_gain,
        w_gate,
        w_up,
        w_down,
    ) = args
    w_gates, w_gate, w_up, stabilizer = w_gates.T, w_gate.T, w_up.T, stabilizer.T
    rows, cols = tokens.shape
    local_heads, seq = stabilizer.shape
    group = kv_size * tp_size
    out_cols = cols // tp_size
    half = local_heads * VD // 2
    vmem = pl.BlockSpec(memory_space=pltpu.VMEM)
    hbm = pl.BlockSpec(memory_space=pl.ANY)
    width = cols * kv_size
    chunks = kv_size

    def like(array):
        return pltpu.VMEM(array.shape, array.dtype)

    results = (
        ((rows, out_cols), BF16),
        (memory.shape, F32),
        (normalizer.shape, F32),
        (stabilizer.shape, F32),
    )
    gains = (mix_gain.reshape(1, cols), mlp_gain.reshape(1, mlp_gain.shape[0]))
    forget_bias = forget_bias.reshape(1, local_heads)
    held = pl.pallas_call(
        functools.partial(layer_kernel, kv_size, tp_size),
        out_shape=tuple(pltpu.VMEM(*result) for result in results),
        in_specs=[hbm] * len(args),
        out_specs=(vmem,) * len(results),
        scratch_shapes=[
            like(w_query),
            like(w_key),
            like(w_value),
            like(w_outgate),
            pltpu.VMEM((w_gates.shape[0], cols), BF16),
            like(tokens),
            like(gains[0]),
            like(forget_bias),
            like(normalizer),
            like(stabilizer),
            like(head_gain),
            like(gains[1]),
            like(w_out),
            like(w_gate),
            like(w_up),
            like(w_down),
            pltpu.VMEM((kv_size, 2 * seq, local_heads * QK), BF16),
            pltpu.VMEM((kv_size, 2 * seq, local_heads * VD), BF16),
            pltpu.VMEM((kv_size, seq, 128), F32),
            pltpu.VMEM((kv_size, 2 * seq, local_heads * QK), BF16),
            pltpu.VMEM((kv_size, 2 * seq, local_heads * VD), BF16),
            pltpu.VMEM((kv_size, seq, 128), F32),
            pltpu.VMEM((kv_size, 2 * seq, half), BF16),
            pltpu.VMEM((rows, cols), BF16),
            pltpu.VMEM((max(tp_size - 1, 1), rows, cols), BF16),
            pltpu.VMEM((kv_size, rows, cols), BF16),
            pltpu.VMEM((kv_size, 1, cols), F32),
            pltpu.VMEM((rows, w_gate.shape[0]), F32),
            pltpu.VMEM((rows, w_up.shape[0]), F32),
            pltpu.VMEM((chunks, rows, width // chunks), BF16),
            pltpu.VMEM((max(tp_size - 1, 1), chunks, rows, width // chunks), BF16),
            pltpu.VMEM((group, rows, out_cols), BF16),
            pltpu.VMEM((kv_size, rows, out_cols), BF16),
            pltpu.SemaphoreType.DMA((10,)),
            pltpu.SemaphoreType.DMA((7,)),
            pltpu.SemaphoreType.DMA((7,)),
            pltpu.SemaphoreType.DMA((3, kv_size - 1)),
            pltpu.SemaphoreType.DMA((kv_size - 1,)),
            pltpu.SemaphoreType.DMA((max(tp_size - 1, 1),)),
            pltpu.SemaphoreType.DMA((kv_size,)),
            pltpu.SemaphoreType.DMA((max(tp_size - 1, 1), chunks)),
            pltpu.SemaphoreType.DMA((kv_size,)),
        ],
        compiler_params=pltpu.CompilerParams(
            collective_id=0, has_side_effects=True, vmem_limit_bytes=48 * 2**20
        ),
    )(*(pltpu.with_memory_space_constraint(x, pltpu.HBM) for x in (
        tokens,
        gains[0],
        w_query,
        w_key,
        w_value,
        w_outgate,
        w_gates,
        forget_bias,
        memory,
        normalizer,
        stabilizer,
        head_gain,
        w_out,
        gains[1],
        w_gate,
        w_up,
        w_down,
    )))
    mixed_out, new_memory, new_normalizer, new_stabilizer = pl.pallas_call(
        store_kernel,
        out_shape=tuple(jax.ShapeDtypeStruct(*result) for result in results),
        in_specs=[vmem] * len(results),
        out_specs=(hbm,) * len(results),
        scratch_shapes=[pltpu.SemaphoreType.DMA((seq + len(results) - 1,))],
        compiler_params=pltpu.CompilerParams(vmem_limit_bytes=2**20),
    )(*held)
    return mixed_out, new_memory, new_normalizer, new_stabilizer.T


def solution(mesh):
    in_specs = (
        P("dp", "kv"),
        P("kv"),
        P("kv", "tp"),
        P("kv", "tp"),
        P("kv", "tp"),
        P("kv", "tp"),
        P(),
        P("tp"),
        P(("dp", "kv"), "tp", None, None),
        P(("dp", "kv"), "tp", None),
        P(("dp", "kv"), "tp"),
        P("tp", None),
        P("tp", "kv"),
        P(),
        P(None, ("kv", "tp")),
        P(None, ("kv", "tp")),
        P(("kv", "tp"), None),
    )
    out_specs = (
        P("dp", ("kv", "tp")),
        P(("dp", "kv"), "tp", None, None),
        P(("dp", "kv"), "tp", None),
        P(("dp", "kv"), "tp"),
    )
    return jax.shard_map(
        functools.partial(body, mesh.shape["kv"], mesh.shape["tp"]),
        mesh=mesh,
        in_specs=in_specs,
        out_specs=out_specs,
        check_vma=False,
    )
```

```python
import functools

import jax
import jax.numpy as jnp
from jax import lax
from jax.experimental import pallas as pl
from jax.experimental.pallas import tpu as pltpu
from jax.sharding import PartitionSpec as P

QK = 128
VD = 256
LANES = 128
EPSILON = 1e-06
MESH = pl.DeviceIdType.MESH
F32 = jnp.float32
BF16 = jnp.bfloat16


def dot(a, b):
    return jnp.dot(a, b, preferred_element_type=F32)


def dot_rows(a, b):
    return lax.dot_general(a, b, (((1,), (1,)), ((), ())), preferred_element_type=F32)


def nearest(rank, me, size):
    inner = jnp.minimum(me, size - 1 - me)
    away = rank // 2 + 1 if rank % 2 else -(rank // 2)
    away = jnp.where(rank <= 2 * inner, away, rank - inner)
    return jnp.where(2 * me < size - 1, me + away, me - away)


def layer_kernel(
    kv_size,
    tp_size,
    tokens_in,
    mix_gain_in,
    w_query,
    w_key,
    w_value,
    w_outgate,
    w_gates,
    forget_bias_in,
    memory,
    normalizer_in,
    stabilizer_in,
    head_gain_in,
    w_out,
    mlp_gain_in,
    w_gate,
    w_up,
    w_down,
    out_mixed,
    vmem,
    out_normalizer,
    out_stabilizer,
    vq,
    vk,
    vv,
    vo,
    vgates,
    tokens,
    mix_gain,
    forget_bias,
    normalizer,
    stabilizer,
    head_gain,
    mlp_gain,
    vwout,
    vgate,
    vup,
    vdown,
    send_qk,
    send_vo,
    send_gs,
    recv_qk,
    recv_vo,
    recv_gs,
    heads_all,
    branch_own,
    branch_recv,
    resid_all,
    gain_rows,
    gate_sum_ref,
    up_sum_ref,
    down_pair,
    pair_recv,
    down_send,
    down_recv,
    load_sem,
    small_sem,
    send_sem,
    recv1,
    recv_gates_sem,
    recv2,
    recv3,
    recv4,
    pair_sem,
    recv5,
):
    me = lax.axis_index("kv")
    core = lax.axis_index("tp")
    rows, cols = tokens.shape
    seq = rows // kv_size
    width = cols * kv_size
    local_heads = forget_bias.shape[1]
    total_heads = local_heads * tp_size
    peers = kv_size - 1
    half = local_heads * VD // 2
    group = kv_size * tp_size
    out_cols = width // group
    lead = tp_size - 1
    sink = 0
    beside_lead = [(lead + 1 + i) % tp_size for i in range(tp_size - 1)]
    beside_sink = [(sink + 1 + i) % tp_size for i in range(tp_size - 1)]
    after_lead = lax.rem(core + tp_size - lead - 1 + tp_size, tp_size)
    after_sink = lax.rem(core + tp_size - sink - 1 + tp_size, tp_size)

    far_first = [nearest(k, me, kv_size) for k in range(kv_size - 1, 0, -1)]
    near_first = far_first[::-1]
    barrier = pltpu.get_barrier_semaphore()
    entered = [{"kv": chip, "tp": other} for chip in far_first for other in range(tp_size)]
    entered += [{"tp": lax.rem(core + step, tp_size)} for step in range(1, tp_size)]
    for device in entered:
        pl.semaphore_signal(barrier, inc=1, device_id=device, device_id_type=MESH)

    loads = [
        pltpu.make_async_copy(src, dst, load_sem.at[i])
        for i, (src, dst) in enumerate(
            (
                (w_gates.at[:, pl.ds(pl.multiple_of(me * cols, cols), cols)], vgates),
                (w_query, vq),
                (w_key, vk),
                (w_value, vv),
                (w_outgate, vo),
                (memory, vmem),
                (w_out, vwout),
                (w_gate, vgate),
                (w_up, vup),
                (w_down, vdown),
            )
        )
    ]
    small = [
        pltpu.make_async_copy(src, dst, small_sem.at[i])
        for i, (src, dst) in enumerate(
            (
                (tokens_in, tokens),
                (mix_gain_in, mix_gain),
                (mlp_gain_in, mlp_gain),
                (forget_bias_in, forget_bias),
                (normalizer_in, normalizer),
                (stabilizer_in, stabilizer),
                (head_gain_in, head_gain),
            )
        )
    ]
    for load in small[:2] + loads[:3]:
        load.start()
    for load in loads[3:5] + small[2:]:
        load.start(priority=1)

    def send(src, dst, index, recv_sem, device):
        pltpu.make_async_remote_copy(
            src_ref=src,
            dst_ref=dst,
            send_sem=send_sem.at[index],
            recv_sem=recv_sem,
            device_id=device,
            device_id_type=MESH,
        ).start()

    def slot(source, target):
        return lax.rem(source - target + kv_size, kv_size) - 1

    def drain(ref, sem):
        pltpu.make_async_copy(ref, ref, sem).wait()

    rising = [jnp.where(chip < me, chip, chip + 1) for chip in range(kv_size - 1)]

    small[0].wait()
    small[1].wait()
    activations = tokens[...].astype(F32)
    square_part = jnp.sum(activations * activations, axis=1, keepdims=True)
    scaled = (activations * mix_gain[...]).astype(BF16)

    def stack_send(target, top, bottom):
        for block in range(kv_size):
            own = slice(block * seq, (block + 1) * seq)
            target[block] = jnp.concatenate([top[own], bottom[own]], axis=0).astype(BF16)

    def scatter(buffer, landing, kind):
        for target in far_first:
            send(buffer.at[target], landing.at[me] if kind else landing.at[slot(me, target)], kind, recv1.at[kind - 1, slot(me, target)] if kind else recv_gates_sem, {"kv": target})

    loads[0].wait()
    gate_part = dot_rows(scaled, vgates[...])
    for block in range(kv_size):
        own = slice(block * seq, (block + 1) * seq)
        send_gs[block, :, 0 : 2 * total_heads] = gate_part[own]
        send_gs[block, :, 2 * total_heads : 2 * total_heads + 1] = square_part[own]
    loads[1].wait()
    query_part = dot(scaled, vq[...])
    loads[2].wait()
    key_part = dot(scaled, vk[...])
    stack_send(send_qk, query_part, key_part)
    pl.semaphore_wait(barrier, group - 1)
    scatter(send_gs, recv_gs, 0)

    @pl.when(core == 0)
    def _():
        scatter(send_qk, recv_qk, 1)

    loads[3].wait()
    value_part = dot(scaled, vv[...])
    loads[4].wait()
    outgate_part = dot(scaled, vo[...])
    stack_send(send_vo, value_part, outgate_part)

    @pl.when(core == 0)
    def _():
        scatter(send_vo, recv_vo, 2)

    for load in loads[5:]:
        load.start()
    for load in small[2:]:
        load.wait()
    for block in range(kv_size):
        gain_rows[block] = mlp_gain[:, block * cols : (block + 1) * cols]

    def total(buffer, landing, kind):
        result = buffer[me].astype(F32)
        for source in near_first:
            drain(landing.at[source], recv1.at[kind - 1, slot(source, me)])
            result = result + landing[source].astype(F32)
        return result

    drain(recv_gs, recv_gates_sem)
    gate_sum = send_gs[me]
    for peer in range(peers):
        gate_sum = gate_sum + recv_gs[peer]

    inverse = lax.rsqrt(gate_sum[:, 2 * total_heads : 2 * total_heads + 1] / width + EPSILON)
    gate_pre = gate_sum[:, : 2 * total_heads] * inverse

    def own_columns(start):
        picked = gate_pre[:, start : start + local_heads]
        for other in range(1, tp_size):
            first = start + other * local_heads
            picked = jnp.where(core == other, gate_pre[:, first : first + local_heads], picked)
        return picked

    input_pre = own_columns(0)
    forget_pre = own_columns(total_heads) + forget_bias[...]
    log_forget = jnp.minimum(forget_pre, 0.0) - jnp.log1p(jnp.exp(-jnp.abs(forget_pre)))
    carried_log = log_forget + stabilizer[...].T
    new_stabilizer = jnp.maximum(carried_log, input_pre)
    out_stabilizer[...] = new_stabilizer.T
    forget_scale = jnp.exp(carried_log - new_stabilizer)
    input_scale = jnp.exp(input_pre - new_stabilizer)

    @pl.when(core != 0)
    def _():
        scatter(send_qk, recv_qk, 1)
        scatter(send_vo, recv_vo, 2)

    qk_sum = total(send_qk, recv_qk, 1)
    query = (qk_sum[:seq] * inverse).astype(BF16).astype(F32)
    key = (qk_sum[seq:] * (inverse * QK ** (-0.5))).astype(BF16).astype(F32)
    loads[5].wait()
    place = lax.broadcasted_iota(jnp.int32, (seq, seq * LANES), 1) // LANES
    spread = jnp.where(
        place == lax.broadcasted_iota(jnp.int32, (seq, seq * LANES), 0), 1.0, 0.0
    ).astype(BF16)
    states = []
    for head in range(local_heads):
        span = slice(head * QK, (head + 1) * QK)
        q, k = query[:, span], key[:, span]
        forget, gain = forget_scale[:, head : head + 1], input_scale[:, head : head + 1]
        scaled_key = gain * k
        new_norm = forget * normalizer[:, head, :] + scaled_key
        out_normalizer[:, head, :] = new_norm
        denominator = jnp.sum(q * new_norm, axis=1, keepdims=True)
        query_key = jnp.sum(q * k, axis=1, keepdims=True)
        q_lanes = dot(q.T.astype(BF16), spread)
        carried = jnp.concatenate(
            [
                jnp.concatenate(
                    [
                        jnp.sum(
                            q_lanes[:, b * LANES : (b + 1) * LANES]
                            * vmem[b, head, :, first : first + LANES],
                            axis=0,
                            keepdims=True,
                        )
                        for first in range(0, VD, LANES)
                    ],
                    axis=1,
                )
                for b in range(seq)
            ],
            axis=0,
        )
        states.append((forget, gain, scaled_key, denominator, query_key, carried))

    vo_sum = total(send_vo, recv_vo, 2)
    values = (vo_sum[:seq] * inverse).astype(BF16).astype(F32)
    outgate = (vo_sum[seq:] * inverse).astype(BF16).astype(F32)
    mixed = []
    for head in range(local_heads):
        forget, gain, scaled_key, denominator, query_key, carried = states[head]
        span = slice(head * VD, (head + 1) * VD)
        numerator = forget * carried + (gain * query_key) * values[:, span]
        head_out = numerator / jnp.maximum(jnp.abs(denominator), 1.0)
        normed = (
            head_out
            * lax.rsqrt(jnp.mean(head_out * head_out, axis=1, keepdims=True) + EPSILON)
            * head_gain[head : head + 1, :]
        )
        mixed.append(normed * jax.nn.sigmoid(outgate[:, span]))
    mixed = jnp.concatenate(mixed, axis=1)
    heads_all[me] = jnp.concatenate([mixed[:, :half], mixed[:, half:]], axis=0).astype(BF16)
    for target in far_first:
        send(heads_all.at[me], heads_all.at[me], 3, recv2, {"kv": target})

    for head in range(local_heads):
        forget, gain, scaled_key, denominator, query_key, carried = states[head]
        k_columns = scaled_key.T
        forget_rows = jnp.broadcast_to(forget, (seq, VD))
        for b in range(seq):
            vmem[b, head] = (
                forget_rows[b : b + 1] * vmem[b, head]
                + k_columns[:, b : b + 1] * values[b : b + 1, head * VD : (head + 1) * VD]
            )

    loads[6].wait()
    drain(heads_all.at[:peers], recv2)
    gathered = [heads_all[block].astype(F32) for block in range(kv_size)]
    low = jnp.concatenate([g[:seq] for g in gathered], axis=0).astype(BF16)
    high = jnp.concatenate([g[seq:] for g in gathered], axis=0).astype(BF16)
    branch_own[...] = (dot(low, vwout[:half, :]) + dot(high, vwout[half:, :])).astype(BF16)

    @pl.when(core != lead)
    def _():
        send(branch_own, branch_recv.at[after_lead], 4, recv3.at[after_lead], {"tp": lead})

    @pl.when(core == lead)
    def _():
        branch = branch_own[...].astype(F32)
        for other in range(len(beside_lead)):
            drain(branch_recv.at[other], recv3.at[other])
            branch = branch + branch_recv[other].astype(F32)
        resid_all[me] = (activations + branch).astype(BF16)
        for target in rising[::-1]:
            send(resid_all.at[me], resid_all.at[me], 4, recv4.at[me], {"kv": target})

    def pass_on(source):
        for other in beside_lead:
            send(
                resid_all.at[source],
                resid_all.at[source],
                5,
                recv4.at[source],
                {"tp": other},
            )

    loads[7].wait()
    loads[8].wait()
    square_sum = 0.0
    for source in [me] + near_first:
        @pl.when(core == lead)
        def _():
            if source is not me:
                drain(resid_all.at[source], recv4.at[source])
            pass_on(source)

        @pl.when(core != lead)
        def _():
            drain(resid_all.at[source], recv4.at[source])

        block = resid_all[source].astype(F32)
        square_sum = square_sum + jnp.sum(block * block, axis=1, keepdims=True)
        block = (block * gain_rows[source]).astype(BF16)
        span = pl.ds(pl.multiple_of(source * cols, cols), cols)
        if source is me:
            gate_sum_ref[...] = dot_rows(block, vgate[:, span])
            up_sum_ref[...] = dot_rows(block, vup[:, span])
        else:
            gate_sum_ref[...] += dot_rows(block, vgate[:, span])
            up_sum_ref[...] += dot_rows(block, vup[:, span])
    inverse_two = lax.rsqrt(square_sum / width + EPSILON)
    gate_value = gate_sum_ref[...] * inverse_two
    up_value = up_sum_ref[...] * inverse_two
    hidden = (gate_value * jax.nn.sigmoid(gate_value) * up_value).astype(BF16)

    loads[9].wait()
    for step, chip in enumerate(rising + [me]):
        span = pl.ds(pl.multiple_of(chip * cols, cols), cols)
        part = dot(hidden, vdown[:, span])

        @pl.when(core != sink)
        def _():
            down_pair[step] = part.astype(BF16)
            send(
                down_pair.at[step],
                pair_recv.at[after_sink, step],
                6,
                pair_sem.at[after_sink, step],
                {"tp": sink},
            )

        @pl.when(core == sink)
        def _():
            summed = part
            for other in range(len(beside_sink)):
                drain(pair_recv.at[other, step], pair_sem.at[other, step])
                summed = summed + pair_recv[other, step].astype(F32)
            for other in range(tp_size):
                first = other * out_cols
                down_send[chip * tp_size + other] = summed[:, first : first + out_cols].astype(BF16)
            if chip is me:
                for other in beside_sink:
                    send(
                        down_send.at[me * tp_size + other],
                        down_recv.at[me],
                        6,
                        recv5.at[me],
                        {"tp": other},
                    )
            else:
                for other in range(tp_size):
                    send(
                        down_send.at[chip * tp_size + other],
                        down_recv.at[me],
                        6,
                        recv5.at[me],
                        {"kv": chip, "tp": other},
                    )

    @pl.when(core == sink)
    def _():
        down_recv[me] = down_send[me * tp_size + sink]

    @pl.when(core != sink)
    def _():
        drain(down_recv.at[me], recv5.at[me])

    residual = resid_all[me].astype(F32)
    summed = down_recv[me].astype(F32) + residual[:, :out_cols]
    if tp_size > 1:
        own_residual = residual[:, :out_cols]
        for other in range(1, tp_size):
            own_residual = jnp.where(
                core == other, residual[:, other * out_cols : (other + 1) * out_cols], own_residual
            )
        summed = down_recv[me].astype(F32) + own_residual
    for source in near_first:
        drain(down_recv.at[source], recv5.at[source])
        summed = summed + down_recv[source].astype(F32)
    out_mixed[...] = summed.astype(BF16)
    drain(send_gs.at[:peers], send_sem.at[0])
    drain(send_qk.at[:peers], send_sem.at[1])
    drain(send_vo.at[:peers], send_sem.at[2])
    drain(heads_all.at[:peers], send_sem.at[3])

    @pl.when(core == lead)
    def _():
        drain(resid_all.at[:peers], send_sem.at[4])
        for _ in range(tp_size - 1):
            drain(resid_all, send_sem.at[5])

    @pl.when(core != lead)
    def _():
        drain(branch_own, send_sem.at[4])

    @pl.when(core == sink)
    def _():
        drain(down_send.at[: group - 1], send_sem.at[6])

    @pl.when(core != sink)
    def _():
        drain(down_pair, send_sem.at[6])


def store_kernel(mixed, memory, normalizer, stabilizer, *rest):
    sem = rest[-1]
    pairs = [(memory.at[i], rest[1].at[i]) for i in range(memory.shape[0])]
    pairs += [(mixed, rest[0]), (normalizer, rest[2]), (stabilizer, rest[3])]
    copies = [
        pltpu.make_async_copy(src, dst, sem.at[i]) for i, (src, dst) in enumerate(pairs)
    ]
    for copy in copies:
        copy.start()
    for copy in copies:
        copy.wait()


def body(kv_size, tp_size, *args):
    (
        tokens,
        mix_gain,
        w_query,
        w_key,
        w_value,
        w_outgate,
        w_gates,
        forget_bias,
        memory,
        normalizer,
        stabilizer,
        head_gain,
        w_out,
        mlp_gain,
        w_gate,
        w_up,
        w_down,
    ) = args
    w_gates, w_gate, w_up, stabilizer = w_gates.T, w_gate.T, w_up.T, stabilizer.T
    rows, cols = tokens.shape
    local_heads, seq = stabilizer.shape
    group = kv_size * tp_size
    out_cols = cols // tp_size
    half = local_heads * VD // 2
    vmem = pl.BlockSpec(memory_space=pltpu.VMEM)
    hbm = pl.BlockSpec(memory_space=pl.ANY)
    width = cols * kv_size
    chunks = kv_size

    def like(array):
        return pltpu.VMEM(array.shape, array.dtype)

    results = (
        ((rows, out_cols), BF16),
        (memory.shape, F32),
        (normalizer.shape, F32),
        (stabilizer.shape, F32),
    )
    gains = (mix_gain.reshape(1, cols), mlp_gain.reshape(1, mlp_gain.shape[0]))
    forget_bias = forget_bias.reshape(1, local_heads)
    held = pl.pallas_call(
        functools.partial(layer_kernel, kv_size, tp_size),
        out_shape=tuple(pltpu.VMEM(*result) for result in results),
        in_specs=[hbm] * len(args),
        out_specs=(vmem,) * len(results),
        scratch_shapes=[
            like(w_query),
            like(w_key),
            like(w_value),
            like(w_outgate),
            pltpu.VMEM((w_gates.shape[0], cols), BF16),
            like(tokens),
            like(gains[0]),
            like(forget_bias),
            like(normalizer),
            like(stabilizer),
            like(head_gain),
            like(gains[1]),
            like(w_out),
            like(w_gate),
            like(w_up),
            like(w_down),
            pltpu.VMEM((kv_size, 2 * seq, local_heads * QK), BF16),
            pltpu.VMEM((kv_size, 2 * seq, local_heads * VD), BF16),
            pltpu.VMEM((kv_size, seq, 128), F32),
            pltpu.VMEM((kv_size, 2 * seq, local_heads * QK), BF16),
            pltpu.VMEM((kv_size, 2 * seq, local_heads * VD), BF16),
            pltpu.VMEM((kv_size - 1, seq, 128), F32),
            pltpu.VMEM((kv_size, 2 * seq, half), BF16),
            pltpu.VMEM((rows, cols), BF16),
            pltpu.VMEM((max(tp_size - 1, 1), rows, cols), BF16),
            pltpu.VMEM((kv_size, rows, cols), BF16),
            pltpu.VMEM((kv_size, 1, cols), F32),
            pltpu.VMEM((rows, w_gate.shape[0]), F32),
            pltpu.VMEM((rows, w_up.shape[0]), F32),
            pltpu.VMEM((chunks, rows, width // chunks), BF16),
            pltpu.VMEM((max(tp_size - 1, 1), chunks, rows, width // chunks), BF16),
            pltpu.VMEM((group, rows, out_cols), BF16),
            pltpu.VMEM((kv_size, rows, out_cols), BF16),
            pltpu.SemaphoreType.DMA((10,)),
            pltpu.SemaphoreType.DMA((7,)),
            pltpu.SemaphoreType.DMA((7,)),
            pltpu.SemaphoreType.DMA((2, kv_size - 1)),
            pltpu.SemaphoreType.DMA,
            pltpu.SemaphoreType.DMA,
            pltpu.SemaphoreType.DMA((max(tp_size - 1, 1),)),
            pltpu.SemaphoreType.DMA((kv_size,)),
            pltpu.SemaphoreType.DMA((max(tp_size - 1, 1), chunks)),
            pltpu.SemaphoreType.DMA((kv_size,)),
        ],
        compiler_params=pltpu.CompilerParams(
            collective_id=0, has_side_effects=True, vmem_limit_bytes=48 * 2**20
        ),
    )(*(pltpu.with_memory_space_constraint(x, pltpu.HBM) for x in (
        tokens,
        gains[0],
        w_query,
        w_key,
        w_value,
        w_outgate,
        w_gates,
        forget_bias,
        memory,
        normalizer,
        stabilizer,
        head_gain,
        w_out,
        gains[1],
        w_gate,
        w_up,
        w_down,
    )))
    mixed_out, new_memory, new_normalizer, new_stabilizer = pl.pallas_call(
        store_kernel,
        out_shape=tuple(jax.ShapeDtypeStruct(*result) for result in results),
        in_specs=[vmem] * len(results),
        out_specs=(hbm,) * len(results),
        scratch_shapes=[pltpu.SemaphoreType.DMA((seq + len(results) - 1,))],
        compiler_params=pltpu.CompilerParams(vmem_limit_bytes=2**20),
    )(*held)
    return mixed_out, new_memory, new_normalizer, new_stabilizer.T


def solution(mesh):
    in_specs = (
        P("dp", "kv"),
        P("kv"),
        P("kv", "tp"),
        P("kv", "tp"),
        P("kv", "tp"),
        P("kv", "tp"),
        P(),
        P("tp"),
        P(("dp", "kv"), "tp", None, None),
        P(("dp", "kv"), "tp", None),
        P(("dp", "kv"), "tp"),
        P("tp", None),
        P("tp", "kv"),
        P(),
        P(None, ("kv", "tp")),
        P(None, ("kv", "tp")),
        P(("kv", "tp"), None),
    )
    out_specs = (
        P("dp", ("kv", "tp")),
        P(("dp", "kv"), "tp", None, None),
        P(("dp", "kv"), "tp", None),
        P(("dp", "kv"), "tp"),
    )
    return jax.shard_map(
        functools.partial(body, mesh.shape["kv"], mesh.shape["tp"]),
        mesh=mesh,
        in_specs=in_specs,
        out_specs=out_specs,
        check_vma=False,
    )
```

```python
import functools

import jax
import jax.numpy as jnp
from jax import lax
from jax.experimental import pallas as pl
from jax.experimental.pallas import tpu as pltpu
from jax.sharding import PartitionSpec as P

QK = 128
VD = 256
LANES = 128
EPSILON = 1e-06
MESH = pl.DeviceIdType.MESH
F32 = jnp.float32
BF16 = jnp.bfloat16


def dot(a, b):
    return jnp.dot(a, b, preferred_element_type=F32)


def dot_rows(a, b):
    return lax.dot_general(a, b, (((1,), (1,)), ((), ())), preferred_element_type=F32)


def nearest(rank, me, size):
    inner = jnp.minimum(me, size - 1 - me)
    away = rank // 2 + 1 if rank % 2 else -(rank // 2)
    away = jnp.where(rank <= 2 * inner, away, rank - inner)
    return jnp.where(2 * me < size - 1, me + away, me - away)


def layer_kernel(
    kv_size,
    tp_size,
    tokens_in,
    mix_gain_in,
    w_query,
    w_key,
    w_value,
    w_outgate,
    w_gates,
    forget_bias_in,
    memory,
    normalizer_in,
    stabilizer_in,
    head_gain_in,
    w_out,
    mlp_gain_in,
    w_gate,
    w_up,
    w_down,
    out_mixed,
    vmem,
    out_normalizer,
    out_stabilizer,
    vq,
    vk,
    vv,
    vo,
    vgates,
    tokens,
    mix_gain,
    forget_bias,
    normalizer,
    stabilizer,
    head_gain,
    mlp_gain,
    vwout,
    vgate,
    vup,
    vdown,
    send_qk,
    send_vo,
    send_gs,
    recv_qk,
    recv_vo,
    recv_gs,
    heads_all,
    branch_own,
    branch_sum,
    branch_recv,
    resid_all,
    gain_rows,
    gate_sum_ref,
    up_sum_ref,
    down_pair,
    pair_recv,
    down_send,
    down_recv,
    load_sem,
    small_sem,
    send_sem,
    recv1,
    recv_gates_sem,
    recv2,
    recv3,
    recv4,
    pair_sem,
    recv5,
):
    me = lax.axis_index("kv")
    core = lax.axis_index("tp")
    rows, cols = tokens.shape
    seq = rows // kv_size
    width = cols * kv_size
    local_heads = forget_bias.shape[1]
    total_heads = local_heads * tp_size
    peers = kv_size - 1
    half = local_heads * VD // 2
    group = kv_size * tp_size
    out_cols = width // group
    lead = tp_size - 1
    sink = 0
    beside_lead = [(lead + 1 + i) % tp_size for i in range(tp_size - 1)]
    beside_sink = [(sink + 1 + i) % tp_size for i in range(tp_size - 1)]
    after_lead = lax.rem(core + tp_size - lead - 1 + tp_size, tp_size)
    after_sink = lax.rem(core + tp_size - sink - 1 + tp_size, tp_size)

    far_first = [nearest(k, me, kv_size) for k in range(kv_size - 1, 0, -1)]
    near_first = far_first[::-1]
    barrier = pltpu.get_barrier_semaphore()
    entered = [{"kv": chip, "tp": other} for chip in far_first for other in range(tp_size)]
    entered += [{"tp": lax.rem(core + step, tp_size)} for step in range(1, tp_size)]
    for device in entered:
        pl.semaphore_signal(barrier, inc=1, device_id=device, device_id_type=MESH)

    loads = [
        pltpu.make_async_copy(src, dst, load_sem.at[i])
        for i, (src, dst) in enumerate(
            (
                (w_gates.at[:, pl.ds(pl.multiple_of(me * cols, cols), cols)], vgates),
                (w_query, vq),
                (w_key, vk),
                (w_value, vv),
                (w_outgate, vo),
                (memory, vmem),
                (w_out, vwout),
                (w_gate, vgate),
                (w_up, vup),
                (w_down, vdown),
            )
        )
    ]
    small = [
        pltpu.make_async_copy(src, dst, small_sem.at[i])
        for i, (src, dst) in enumerate(
            (
                (tokens_in, tokens),
                (mix_gain_in, mix_gain),
                (mlp_gain_in, mlp_gain),
                (forget_bias_in, forget_bias),
                (normalizer_in, normalizer),
                (stabilizer_in, stabilizer),
                (head_gain_in, head_gain),
            )
        )
    ]
    for load in small[:2] + loads[:3]:
        load.start()
    for load in loads[3:5] + small[2:]:
        load.start(priority=1)

    def send(src, dst, index, recv_sem, device):
        pltpu.make_async_remote_copy(
            src_ref=src,
            dst_ref=dst,
            send_sem=send_sem.at[index],
            recv_sem=recv_sem,
            device_id=device,
            device_id_type=MESH,
        ).start()

    def slot(source, target):
        return lax.rem(source - target + kv_size, kv_size) - 1

    def drain(ref, sem):
        pltpu.make_async_copy(ref, ref, sem).wait()

    rising = [jnp.where(chip < me, chip, chip + 1) for chip in range(kv_size - 1)]

    small[0].wait()
    small[1].wait()
    activations = tokens[...].astype(F32)
    square_part = jnp.sum(activations * activations, axis=1, keepdims=True)
    scaled = (activations * mix_gain[...]).astype(BF16)

    def stack_send(target, top, bottom):
        for block in range(kv_size):
            own = slice(block * seq, (block + 1) * seq)
            target[block] = jnp.concatenate([top[own], bottom[own]], axis=0).astype(BF16)

    def scatter(buffer, landing, kind):
        for target in far_first:
            send(buffer.at[target], landing.at[me] if kind else landing.at[slot(me, target)], kind, recv1.at[kind - 1, slot(me, target)] if kind else recv_gates_sem, {"kv": target})

    loads[0].wait()
    gate_part = dot_rows(scaled, vgates[...])
    for block in range(kv_size):
        own = slice(block * seq, (block + 1) * seq)
        send_gs[block, :, 0 : 2 * total_heads] = gate_part[own]
        send_gs[block, :, 2 * total_heads : 2 * total_heads + 1] = square_part[own]
    loads[1].wait()
    query_part = dot(scaled, vq[...])
    loads[2].wait()
    key_part = dot(scaled, vk[...])
    stack_send(send_qk, query_part, key_part)
    pl.semaphore_wait(barrier, group - 1)
    scatter(send_gs, recv_gs, 0)

    @pl.when(core == 0)
    def _():
        scatter(send_qk, recv_qk, 1)

    loads[3].wait()
    value_part = dot(scaled, vv[...])
    loads[4].wait()
    outgate_part = dot(scaled, vo[...])
    stack_send(send_vo, value_part, outgate_part)

    @pl.when(core == 0)
    def _():
        scatter(send_vo, recv_vo, 2)

    for load in loads[5:]:
        load.start()
    for load in small[2:]:
        load.wait()
    for block in range(kv_size):
        gain_rows[block] = mlp_gain[:, block * cols : (block + 1) * cols]

    def total(buffer, landing, kind):
        result = buffer[me].astype(F32)
        for source in near_first:
            drain(landing.at[source], recv1.at[kind - 1, slot(source, me)])
            result = result + landing[source].astype(F32)
        return result

    drain(recv_gs, recv_gates_sem)
    gate_sum = send_gs[me]
    for peer in range(peers):
        gate_sum = gate_sum + recv_gs[peer]

    inverse = lax.rsqrt(gate_sum[:, 2 * total_heads : 2 * total_heads + 1] / width + EPSILON)
    gate_pre = gate_sum[:, : 2 * total_heads] * inverse

    def own_columns(start):
        picked = gate_pre[:, start : start + local_heads]
        for other in range(1, tp_size):
            first = start + other * local_heads
            picked = jnp.where(core == other, gate_pre[:, first : first + local_heads], picked)
        return picked

    input_pre = own_columns(0)
    forget_pre = own_columns(total_heads) + forget_bias[...]
    log_forget = jnp.minimum(forget_pre, 0.0) - jnp.log1p(jnp.exp(-jnp.abs(forget_pre)))
    carried_log = log_forget + stabilizer[...].T
    new_stabilizer = jnp.maximum(carried_log, input_pre)
    out_stabilizer[...] = new_stabilizer.T
    forget_scale = jnp.exp(carried_log - new_stabilizer)
    input_scale = jnp.exp(input_pre - new_stabilizer)

    @pl.when(core != 0)
    def _():
        scatter(send_qk, recv_qk, 1)
        scatter(send_vo, recv_vo, 2)

    qk_sum = total(send_qk, recv_qk, 1)
    query = (qk_sum[:seq] * inverse).astype(BF16).astype(F32)
    key = (qk_sum[seq:] * (inverse * QK ** (-0.5))).astype(BF16).astype(F32)
    loads[5].wait()
    place = lax.broadcasted_iota(jnp.int32, (seq, seq * LANES), 1) // LANES
    spread = jnp.where(
        place == lax.broadcasted_iota(jnp.int32, (seq, seq * LANES), 0), 1.0, 0.0
    ).astype(BF16)
    states = []
    for head in range(local_heads):
        span = slice(head * QK, (head + 1) * QK)
        q, k = query[:, span], key[:, span]
        forget, gain = forget_scale[:, head : head + 1], input_scale[:, head : head + 1]
        scaled_key = gain * k
        new_norm = forget * normalizer[:, head, :] + scaled_key
        out_normalizer[:, head, :] = new_norm
        denominator = jnp.sum(q * new_norm, axis=1, keepdims=True)
        query_key = jnp.sum(q * k, axis=1, keepdims=True)
        q_lanes = dot(q.T.astype(BF16), spread)
        carried = jnp.concatenate(
            [
                jnp.concatenate(
                    [
                        jnp.sum(
                            q_lanes[:, b * LANES : (b + 1) * LANES]
                            * vmem[b, head, :, first : first + LANES],
                            axis=0,
                            keepdims=True,
                        )
                        for first in range(0, VD, LANES)
                    ],
                    axis=1,
                )
                for b in range(seq)
            ],
            axis=0,
        )
        states.append((forget, gain, scaled_key, denominator, query_key, carried))

    vo_sum = total(send_vo, recv_vo, 2)
    values = (vo_sum[:seq] * inverse).astype(BF16).astype(F32)
    outgate = (vo_sum[seq:] * inverse).astype(BF16).astype(F32)
    mixed = []
    for head in range(local_heads):
        forget, gain, scaled_key, denominator, query_key, carried = states[head]
        span = slice(head * VD, (head + 1) * VD)
        numerator = forget * carried + (gain * query_key) * values[:, span]
        head_out = numerator / jnp.maximum(jnp.abs(denominator), 1.0)
        normed = (
            head_out
            * lax.rsqrt(jnp.mean(head_out * head_out, axis=1, keepdims=True) + EPSILON)
            * head_gain[head : head + 1, :]
        )
        mixed.append(normed * jax.nn.sigmoid(outgate[:, span]))
        if (head + 1) * VD % half == 0:
            part = (head + 1) * VD // half - 1
            heads_all[part, me] = jnp.concatenate(mixed, axis=1).astype(BF16)
            mixed = []
            for target in far_first:
                send(
                    heads_all.at[part, me],
                    heads_all.at[part, me],
                    3,
                    recv2.at[part],
                    {"kv": target},
                )

    for head in range(local_heads):
        forget, gain, scaled_key, denominator, query_key, carried = states[head]
        k_columns = scaled_key.T
        forget_rows = jnp.broadcast_to(forget, (seq, VD))
        for b in range(seq):
            vmem[b, head] = (
                forget_rows[b : b + 1] * vmem[b, head]
                + k_columns[:, b : b + 1] * values[b : b + 1, head * VD : (head + 1) * VD]
            )

    loads[6].wait()
    for part in range(2):
        drain(heads_all.at[part, :peers], recv2.at[part])
        gathered = [heads_all[part, block].astype(F32) for block in range(kv_size)]
        gathered = jnp.concatenate(gathered, axis=0).astype(BF16)
        if part == 0:
            branch_sum[...] = dot(gathered, vwout[:half, :])
        else:
            branch_own[...] = (branch_sum[...] + dot(gathered, vwout[half:, :])).astype(BF16)

    @pl.when(core != lead)
    def _():
        send(branch_own, branch_recv.at[after_lead], 4, recv3.at[after_lead], {"tp": lead})

    @pl.when(core == lead)
    def _():
        branch = branch_own[...].astype(F32)
        for other in range(len(beside_lead)):
            drain(branch_recv.at[other], recv3.at[other])
            branch = branch + branch_recv[other].astype(F32)
        resid_all[me] = (activations + branch).astype(BF16)
        for target in rising[::-1]:
            send(resid_all.at[me], resid_all.at[me], 4, recv4.at[me], {"kv": target})

    def pass_on(source):
        for other in beside_lead:
            send(
                resid_all.at[source],
                resid_all.at[source],
                5,
                recv4.at[source],
                {"tp": other},
            )

    loads[7].wait()
    loads[8].wait()
    square_sum = 0.0
    for source in [me] + near_first:
        @pl.when(core == lead)
        def _():
            if source is not me:
                drain(resid_all.at[source], recv4.at[source])
            pass_on(source)

        @pl.when(core != lead)
        def _():
            drain(resid_all.at[source], recv4.at[source])

        block = resid_all[source].astype(F32)
        square_sum = square_sum + jnp.sum(block * block, axis=1, keepdims=True)
        block = (block * gain_rows[source]).astype(BF16)
        span = pl.ds(pl.multiple_of(source * cols, cols), cols)
        if source is me:
            gate_sum_ref[...] = dot_rows(block, vgate[:, span])
            up_sum_ref[...] = dot_rows(block, vup[:, span])
        else:
            gate_sum_ref[...] += dot_rows(block, vgate[:, span])
            up_sum_ref[...] += dot_rows(block, vup[:, span])
    inverse_two = lax.rsqrt(square_sum / width + EPSILON)
    gate_value = gate_sum_ref[...] * inverse_two
    up_value = up_sum_ref[...] * inverse_two
    hidden = (gate_value * jax.nn.sigmoid(gate_value) * up_value).astype(BF16)

    loads[9].wait()
    for step, chip in enumerate(rising + [me]):
        span = pl.ds(pl.multiple_of(chip * cols, cols), cols)
        part = dot(hidden, vdown[:, span])

        @pl.when(core != sink)
        def _():
            down_pair[step] = part.astype(BF16)
            send(
                down_pair.at[step],
                pair_recv.at[after_sink, step],
                6,
                pair_sem.at[after_sink, step],
                {"tp": sink},
            )

        @pl.when(core == sink)
        def _():
            summed = part
            for other in range(len(beside_sink)):
                drain(pair_recv.at[other, step], pair_sem.at[other, step])
                summed = summed + pair_recv[other, step].astype(F32)
            for other in range(tp_size):
                first = other * out_cols
                down_send[chip * tp_size + other] = summed[:, first : first + out_cols].astype(BF16)
            if chip is me:
                for other in beside_sink:
                    send(
                        down_send.at[me * tp_size + other],
                        down_recv.at[me],
                        6,
                        recv5.at[me],
                        {"tp": other},
                    )
            else:
                for other in range(tp_size):
                    send(
                        down_send.at[chip * tp_size + other],
                        down_recv.at[me],
                        6,
                        recv5.at[me],
                        {"kv": chip, "tp": other},
                    )

    @pl.when(core == sink)
    def _():
        down_recv[me] = down_send[me * tp_size + sink]

    @pl.when(core != sink)
    def _():
        drain(down_recv.at[me], recv5.at[me])

    residual = resid_all[me].astype(F32)
    summed = down_recv[me].astype(F32) + residual[:, :out_cols]
    if tp_size > 1:
        own_residual = residual[:, :out_cols]
        for other in range(1, tp_size):
            own_residual = jnp.where(
                core == other, residual[:, other * out_cols : (other + 1) * out_cols], own_residual
            )
        summed = down_recv[me].astype(F32) + own_residual
    for source in near_first:
        drain(down_recv.at[source], recv5.at[source])
        summed = summed + down_recv[source].astype(F32)
    out_mixed[...] = summed.astype(BF16)
    drain(send_gs.at[:peers], send_sem.at[0])
    drain(send_qk.at[:peers], send_sem.at[1])
    drain(send_vo.at[:peers], send_sem.at[2])
    drain(heads_all.at[:, :peers], send_sem.at[3])

    @pl.when(core == lead)
    def _():
        drain(resid_all.at[:peers], send_sem.at[4])
        for _ in range(tp_size - 1):
            drain(resid_all, send_sem.at[5])

    @pl.when(core != lead)
    def _():
        drain(branch_own, send_sem.at[4])

    @pl.when(core == sink)
    def _():
        drain(down_send.at[: group - 1], send_sem.at[6])

    @pl.when(core != sink)
    def _():
        drain(down_pair, send_sem.at[6])


def store_kernel(mixed, memory, normalizer, stabilizer, *rest):
    sem = rest[-1]
    pairs = [(memory.at[i], rest[1].at[i]) for i in range(memory.shape[0])]
    pairs += [(mixed, rest[0]), (normalizer, rest[2]), (stabilizer, rest[3])]
    copies = [
        pltpu.make_async_copy(src, dst, sem.at[i]) for i, (src, dst) in enumerate(pairs)
    ]
    for copy in copies:
        copy.start()
    for copy in copies:
        copy.wait()


def body(kv_size, tp_size, *args):
    (
        tokens,
        mix_gain,
        w_query,
        w_key,
        w_value,
        w_outgate,
        w_gates,
        forget_bias,
        memory,
        normalizer,
        stabilizer,
        head_gain,
        w_out,
        mlp_gain,
        w_gate,
        w_up,
        w_down,
    ) = args
    w_gates, w_gate, w_up, stabilizer = w_gates.T, w_gate.T, w_up.T, stabilizer.T
    rows, cols = tokens.shape
    local_heads, seq = stabilizer.shape
    group = kv_size * tp_size
    out_cols = cols // tp_size
    half = local_heads * VD // 2
    vmem = pl.BlockSpec(memory_space=pltpu.VMEM)
    hbm = pl.BlockSpec(memory_space=pl.ANY)
    width = cols * kv_size
    chunks = kv_size

    def like(array):
        return pltpu.VMEM(array.shape, array.dtype)

    results = (
        ((rows, out_cols), BF16),
        (memory.shape, F32),
        (normalizer.shape, F32),
        (stabilizer.shape, F32),
    )
    gains = (mix_gain.reshape(1, cols), mlp_gain.reshape(1, mlp_gain.shape[0]))
    forget_bias = forget_bias.reshape(1, local_heads)
    held = pl.pallas_call(
        functools.partial(layer_kernel, kv_size, tp_size),
        out_shape=tuple(pltpu.VMEM(*result) for result in results),
        in_specs=[hbm] * len(args),
        out_specs=(vmem,) * len(results),
        scratch_shapes=[
            like(w_query),
            like(w_key),
            like(w_value),
            like(w_outgate),
            pltpu.VMEM((w_gates.shape[0], cols), BF16),
            like(tokens),
            like(gains[0]),
            like(forget_bias),
            like(normalizer),
            like(stabilizer),
            like(head_gain),
            like(gains[1]),
            like(w_out),
            like(w_gate),
            like(w_up),
            like(w_down),
            pltpu.VMEM((kv_size, 2 * seq, local_heads * QK), BF16),
            pltpu.VMEM((kv_size, 2 * seq, local_heads * VD), BF16),
            pltpu.VMEM((kv_size, seq, 128), F32),
            pltpu.VMEM((kv_size, 2 * seq, local_heads * QK), BF16),
            pltpu.VMEM((kv_size, 2 * seq, local_heads * VD), BF16),
            pltpu.VMEM((kv_size - 1, seq, 128), F32),
            pltpu.VMEM((2, kv_size, seq, half), BF16),
            pltpu.VMEM((rows, cols), BF16),
            pltpu.VMEM((rows, cols), F32),
            pltpu.VMEM((max(tp_size - 1, 1), rows, cols), BF16),
            pltpu.VMEM((kv_size, rows, cols), BF16),
            pltpu.VMEM((kv_size, 1, cols), F32),
            pltpu.VMEM((rows, w_gate.shape[0]), F32),
            pltpu.VMEM((rows, w_up.shape[0]), F32),
            pltpu.VMEM((chunks, rows, width // chunks), BF16),
            pltpu.VMEM((max(tp_size - 1, 1), chunks, rows, width // chunks), BF16),
            pltpu.VMEM((group, rows, out_cols), BF16),
            pltpu.VMEM((kv_size, rows, out_cols), BF16),
            pltpu.SemaphoreType.DMA((10,)),
            pltpu.SemaphoreType.DMA((7,)),
            pltpu.SemaphoreType.DMA((7,)),
            pltpu.SemaphoreType.DMA((2, kv_size - 1)),
            pltpu.SemaphoreType.DMA,
            pltpu.SemaphoreType.DMA((2,)),
            pltpu.SemaphoreType.DMA((max(tp_size - 1, 1),)),
            pltpu.SemaphoreType.DMA((kv_size,)),
            pltpu.SemaphoreType.DMA((max(tp_size - 1, 1), chunks)),
            pltpu.SemaphoreType.DMA((kv_size,)),
        ],
        compiler_params=pltpu.CompilerParams(
            collective_id=0, has_side_effects=True, vmem_limit_bytes=48 * 2**20
        ),
    )(*(pltpu.with_memory_space_constraint(x, pltpu.HBM) for x in (
        tokens,
        gains[0],
        w_query,
        w_key,
        w_value,
        w_outgate,
        w_gates,
        forget_bias,
        memory,
        normalizer,
        stabilizer,
        head_gain,
        w_out,
        gains[1],
        w_gate,
        w_up,
        w_down,
    )))
    mixed_out, new_memory, new_normalizer, new_stabilizer = pl.pallas_call(
        store_kernel,
        out_shape=tuple(jax.ShapeDtypeStruct(*result) for result in results),
        in_specs=[vmem] * len(results),
        out_specs=(hbm,) * len(results),
        scratch_shapes=[pltpu.SemaphoreType.DMA((seq + len(results) - 1,))],
        compiler_params=pltpu.CompilerParams(vmem_limit_bytes=2**20),
    )(*held)
    return mixed_out, new_memory, new_normalizer, new_stabilizer.T


def solution(mesh):
    in_specs = (
        P("dp", "kv"),
        P("kv"),
        P("kv", "tp"),
        P("kv", "tp"),
        P("kv", "tp"),
        P("kv", "tp"),
        P(),
        P("tp"),
        P(("dp", "kv"), "tp", None, None),
        P(("dp", "kv"), "tp", None),
        P(("dp", "kv"), "tp"),
        P("tp", None),
        P("tp", "kv"),
        P(),
        P(None, ("kv", "tp")),
        P(None, ("kv", "tp")),
        P(("kv", "tp"), None),
    )
    out_specs = (
        P("dp", ("kv", "tp")),
        P(("dp", "kv"), "tp", None, None),
        P(("dp", "kv"), "tp", None),
        P(("dp", "kv"), "tp"),
    )
    return jax.shard_map(
        functools.partial(body, mesh.shape["kv"], mesh.shape["tp"]),
        mesh=mesh,
        in_specs=in_specs,
        out_specs=out_specs,
        check_vma=False,
    )
```
